256 devices in a mesh: grp: 2 (over y), sp: 16 (over z), tp: 8 (over x, core).
Axes of the slice: x: 4, y: 2, z: 16, core: 2. Of those that a mesh axis runs over, the one named last changes fastest.
The devices are a block of a 4x16x16 slice.
Arguments:
- layer_feed: bfloat16 [4, 8192, 4096], P('grp', 'sp'), parts along dimension 0, may hold values from -13 to 13
- address_mapping: bfloat16 [4096, 2048], P(None, 'tp'), may hold values from -0.09375 to 0.09375
- content_mapping: bfloat16 [4096, 2048], P(None, 'tp'), may hold values from -0.09375 to 0.09375
- beta_mapping_matrix: bfloat16 [4096, 32], replicated, may hold values from -0.032958984 to 0.029541016
- forgetting_mapping: bfloat16 [4096, 32], replicated, may hold values from -0.09375 to 0.09375
- logged_fading_speed: float32 [32], P('tp'), may hold values from -12 to -2.8
- extra_forgetting: bfloat16 [4, 8192, 32], P('grp', 'sp', 'tp'), parts along dimension 0, may hold values from -1.4 to 0
- opening_probe: bfloat16 [4, 2048], P('grp', 'tp'), parts along dimension 0, may hold values from -6 to 6
Outputs:
- context_memory_tensor: bfloat16 [4, 32, 64, 64], P('grp', 'tp', 'sp'), parts along dimension 0
- opening_normed_output: bfloat16 [4, 2048], P('grp', 'tp'), parts along dimension 0
The draws below stay inside these ranges and needn't reach their ends.
There are 2 independent parts, one for each index of `grp`. The reference program is written for one: setup_inputs(seed, part) draws one part's arguments, and reference() takes and returns one part's arrays. A program takes and returns all parts, laid end to end along the dimension named above; an argument that names none is the same for every part. Nothing has to cross between parts.
All inputs are finite; a program needn't handle non-finite values.
Results may differ from the reference program's by a relative error of at most 0.014.
Values sent between devices are 32-bit elements; how exact they have to be, the bound alone decides.
No kernel may reach another device: no remote copies, remote signals or barrier semaphores. Data moves between devices by JAX's collectives and lax.ppermute only.
A program may use at most 64 MiB of HBM per device.

```python
import math
import jax
import jax.numpy as jnp
from jax import lax

D = 4096
H = 32
HEAD = 64
SEQS = 2
TOK_DEV = 1024
LEN = 8192


def draw_layer_feed(key, part):
    span = TOK_DEV // SEQS
    count = LEN // span
    normal_key = jax.random.fold_in(key, 11)
    scale_key = jax.random.fold_in(key, 12)
    shift_key = jax.random.fold_in(key, 13)
    base = jnp.clip(jax.random.normal(normal_key, (SEQS, count, span, D), jnp.float32), -4.0, 4.0)
    levels = jnp.exp(jax.random.uniform(scale_key, (SEQS, count, 1, 1), jnp.float32, math.log(0.3), math.log(3.0)))
    shifts = jax.random.uniform(shift_key, (SEQS, 1, 1, 1), jnp.float32, 0.45, 0.55)
    scaled = base * levels + shifts
    return scaled.reshape(SEQS, LEN, D).astype(jnp.bfloat16)


def draw_beta_mapping_matrix(key, part):
    noise_key = jax.random.fold_in(key, 41)
    noise = jnp.clip(jax.random.normal(noise_key, (D, H), jnp.float32), -4.0, 4.0) * 0.5
    return (noise * D ** (-0.5) - 7.0 / D).astype(jnp.bfloat16)


def draw_logged_fading_speed(key, part):
    pick_key = jax.random.fold_in(key, 21)
    slow_key = jax.random.fold_in(key, 22)
    fast_key = jax.random.fold_in(key, 23)
    fast = jax.random.bernoulli(pick_key, 0.5, (H,))
    slow_rate = jax.random.uniform(slow_key, (H,), jnp.float32, 0.1, 0.5) / LEN
    fast_rate = jnp.exp(jax.random.uniform(fast_key, (H,), jnp.float32, math.log(0.03), math.log(0.06)))
    return jnp.log(jnp.where(fast, fast_rate, slow_rate)).astype(jnp.float32)


def draw_extra_forgetting(key, part):
    place_key = jax.random.fold_in(key, 31)
    depth_key = jax.random.fold_in(key, 32)
    spots = jax.random.randint(place_key, (SEQS, 2, 1, H), 0, LEN)
    depths = jnp.log(jax.random.uniform(depth_key, (SEQS, 2, 1, H), jnp.float32, 0.5, 0.8))
    positions = jnp.arange(LEN)[None, None, :, None]
    total = jnp.sum(jnp.where(positions == spots, depths, 0.0), axis=1)
    return total.astype(jnp.bfloat16)


def block_scale(stream_key, shape, cuts, low, top_value):
    loudness = 1.0
    for position, blocks in cuts:
        heights = jax.random.uniform(jax.random.fold_in(jax.random.fold_in(stream_key, 6), position), (blocks,), jnp.float32, low / len(cuts), top_value / len(cuts))
        loudness = loudness * jnp.repeat(jnp.exp(heights), shape[position] // blocks).reshape((-1,) + (1,) * (len(shape) - 1 - position))
    return loudness


def centred(rng, shape, spread, reach, shards=(), held_as=jnp.bfloat16):
    array = spread * jax.random.normal(rng, shape, jnp.float32)
    if shards:
        array = array * block_scale(rng, shape, shards, -0.22, 0.18)
    return jnp.clip(array, -reach, reach).astype(held_as)


def setup_inputs(seed: int = 0, part: int = 0) -> dict:
    streams_of = jax.random.split(jax.random.key(seed), 9)
    part_keys = jax.random.split(jax.random.fold_in(streams_of[8], part), 9)
    layer_feed = draw_layer_feed(jax.random.fold_in(jax.random.fold_in(streams_of[8], part), 71), part)
    address_mapping = centred(streams_of[1], (D, H * HEAD), D ** -0.5, 0.09375, ((1, 8),))
    content_mapping = centred(streams_of[2], (D, H * HEAD), D ** -0.5, 0.09375, ((1, 8),))
    beta_mapping_matrix = draw_beta_mapping_matrix(jax.random.fold_in(streams_of[8], 71), part)
    forgetting_mapping = centred(streams_of[4], (D, H), D ** -0.5, 0.09375)
    logged_fading_speed = draw_logged_fading_speed(jax.random.fold_in(streams_of[8], 71), part)
    extra_forgetting = draw_extra_forgetting(jax.random.fold_in(jax.random.fold_in(streams_of[8], part), 71), part)
    opening_probe = centred(part_keys[7], (SEQS, H * HEAD), 1.0, 6.0, ((1, 8),))
    return dict(layer_feed=layer_feed, address_mapping=address_mapping, content_mapping=content_mapping, beta_mapping_matrix=beta_mapping_matrix, forgetting_mapping=forgetting_mapping, logged_fading_speed=logged_fading_speed, extra_forgetting=extra_forgetting, opening_probe=opening_probe)


def reference(layer_feed, address_mapping, content_mapping, beta_mapping_matrix, forgetting_mapping, logged_fading_speed, extra_forgetting, opening_probe):

    def lone_example(input_tokens):
        sequence_tokens, sequence_batch, sequence_query = input_tokens
        address_embeddings = jnp.dot(sequence_tokens, address_mapping, preferred_element_type=jnp.float32).astype(jnp.bfloat16)
        content_embeddings = jnp.dot(sequence_tokens, content_mapping, preferred_element_type=jnp.float32).astype(jnp.bfloat16)
        beta_raw_scores = jnp.dot(sequence_tokens, beta_mapping_matrix, preferred_element_type=jnp.float32).astype(jnp.bfloat16)
        forgetting_raw_scores = jnp.dot(sequence_tokens, forgetting_mapping, preferred_element_type=jnp.float32).astype(jnp.bfloat16)
        keys = jax.nn.silu(address_embeddings.astype(jnp.float32)).reshape(-1, H, HEAD)
        keys = keys * lax.rsqrt(lax.optimization_barrier(jnp.sum(keys * keys, axis=-1, keepdims=True)) + 1e-06)
        values = jax.nn.silu(content_embeddings.astype(jnp.float32)).reshape(-1, H, HEAD)
        betas = jax.nn.sigmoid(beta_raw_scores.astype(jnp.float32))
        decay_factors = -jnp.exp(logged_fading_speed) * jax.nn.softplus(forgetting_raw_scores.astype(jnp.float32)) + sequence_batch.astype(jnp.float32)

        def advance(state, items):
            key_vector_row, value_row, beta_row, gamma_row = items
            retained = jnp.exp(gamma_row)[:, None, None] * state
            estimate = jnp.einsum('yz,yzt->yt', key_vector_row, retained, precision=lax.Precision.HIGHEST)
            state = retained + (beta_row[:, None] * key_vector_row)[:, :, None] * (value_row - estimate)[:, None, :]
            return (state, None)
        start = jnp.zeros((H, HEAD, HEAD), jnp.float32)
        final, _ = lax.scan(advance, start, (keys, values, betas, decay_factors))
        state_store = final.astype(jnp.bfloat16)
        query_per_head = sequence_query.astype(jnp.float32).reshape(H, HEAD)
        state_readout = jnp.einsum('yz,yzt->yt', query_per_head, final, precision=lax.Precision.HIGHEST)
        state_readout = state_readout * lax.rsqrt(lax.optimization_barrier(jnp.mean(state_readout * state_readout, axis=-1, keepdims=True)) + 1e-06)
        return (state_store, state_readout.reshape(H * HEAD).astype(jnp.bfloat16))
    context_memory_tensor, opening_normed_output = lax.map(lone_example, (layer_feed, extra_forgetting, opening_probe))
    return (context_memory_tensor, opening_normed_output)
```

```python
import functools

import jax
import jax.numpy as jnp
from jax import lax
from jax.experimental import pallas as pl
from jax.experimental.pallas import tpu as pltpu
from jax.sharding import PartitionSpec as P

HEAD = 64
BASE = 8
F32 = jnp.float32
BF16 = jnp.bfloat16


def iota(shape, dim):
    return lax.broadcasted_iota(jnp.int32, shape, dim)


def silu(v):
    return v / (1.0 + jnp.exp(-v))


def dot(a, b, dims=(1, 0)):
    return lax.dot_general(a, b, (((dims[0],), (dims[1],)), ((), ())), preferred_element_type=F32)


def lanes_turned(x, amount):
    amount %= x.shape[1]
    return pltpu.roll(x, amount, 1) if amount else x


def block_diagonal(x, mask):
    return jnp.tile(x, (mask.shape[0] // x.shape[0], 1)) * mask


def running_sum(x):
    rows = iota(x.shape, 0)
    step = 1
    while step < x.shape[0]:
        x = x + jnp.where(rows >= step, pltpu.roll(x, step, 0), 0.0)
        step *= 2
    return x


def small_inverse(lower, heads):
    width = lower.shape[1]
    column = iota((BASE, width), 1) % HEAD
    blocks = jnp.zeros((BASE, width), F32)
    for r in range(HEAD // BASE):
        blocks = jnp.where(column // BASE == r, lower[BASE * r : BASE * (r + 1)], blocks)
    inverse = jnp.where(iota((BASE, width), 0) == column % BASE, 1.0, 0.0)
    lane = iota((BASE, 128), 1)
    pieces = []
    for first in range(0, width, 128):
        part, x = blocks[:, first : first + 128], inverse[:, first : first + 128]
        for m in range(BASE - 1):
            factor = jnp.take_along_axis(part, lane // BASE * BASE + m, axis=1)
            x = x - factor * x[m : m + 1]
        pieces.append(x)
    inverse = jnp.concatenate(pieces, axis=1)
    return jnp.concatenate(
        [jnp.where(column // BASE == r, inverse, 0.0) for r in range(HEAD // BASE)], axis=0
    )


def chunk_map(k, v, beta, total, mask, heads):
    width = heads * HEAD
    row, column = iota((HEAD, width), 0), iota((HEAD, width), 1) % HEAD
    eye = row == column
    across = jnp.sum(jnp.where(eye, total, 0.0), axis=0, keepdims=True)
    last = total[HEAD - 1 :]
    low = k.astype(BF16)
    gram = dot(low, block_diagonal(low, mask), (1, 1))
    lower = jnp.where(row > column, beta * gram * jnp.exp(jnp.minimum(total - across, 0.0)), 0.0)
    inverse = small_inverse(lower, heads)
    size = BASE
    while size < HEAD:
        here = (row // (2 * size) == column // (2 * size)) & (row // size > column // size)
        off = jnp.where(here, lower, 0.0).astype(BF16)
        rounded = inverse.astype(BF16)
        inner = dot(off, block_diagonal(rounded, mask))
        inverse = inverse - dot(rounded, block_diagonal(inner.astype(BF16), mask))
        size *= 2
    carried = k * jnp.exp(last - total)
    turned = carried.T
    turned = jnp.concatenate(
        [turned[HEAD * h : HEAD * (h + 1)] for h in range(heads)], axis=1
    ).astype(BF16)
    closing = dot(turned, block_diagonal(inverse.astype(BF16), mask)).astype(BF16)
    taken = (k * (beta * jnp.exp(total))).astype(BF16)
    added = (v * beta).astype(BF16)
    removal = dot(closing, block_diagonal(taken, mask))
    removal = removal + jnp.where(eye, 1.0 - jnp.exp(last), 0.0)
    return removal, dot(closing, block_diagonal(added, mask))


def after(later, earlier, mask):
    r2, o2 = later
    r1, o1 = earlier
    low = r2.astype(BF16)
    return (
        r1 + r2 - dot(low, block_diagonal(r1.astype(BF16), mask)),
        o1 + o2 - dot(low, block_diagonal(o1.astype(BF16), mask)),
    )


def composed(parts, combine):
    while len(parts) > 1:
        joined = [combine(parts[i + 1], parts[i]) for i in range(0, len(parts) - 1, 2)]
        parts = joined + parts[len(joined) * 2 :]
    return parts[0]


def local_kernel(
    heads, seqs, length, place_ref, speed_ref, x_ref, wk_ref, wv_ref, wb_ref, wf_ref, extra_ref, out_ref,
    kv_acc, small_acc, mask_ref, k_ref, v_ref, beta_ref, total_ref
):
    step = pl.program_id(0)
    width = heads * HEAD
    all_heads = wb_ref.shape[1]

    @pl.when(step == 0)
    def _():
        kv_acc[...] = jnp.zeros_like(kv_acc)
        small_acc[...] = jnp.zeros_like(small_acc)

    x = x_ref[...]
    kv_acc[:, :width] += dot(x, wk_ref[...])
    kv_acc[:, width:] += dot(x, wv_ref[...])
    small_acc[...] += dot(x, jnp.concatenate([wb_ref[...], wf_ref[...]], axis=1))

    @pl.when(step == pl.num_programs(0) - 1)
    def _():
        rows, cols = iota((width, width), 0), iota((width, width), 1)
        mask_ref[...] = jnp.where(rows // HEAD == cols // HEAD, 1.0, 0.0).astype(BF16)
        mask = mask_ref[...]
        first = place_ref[0] * heads
        pick_row, pick_col = iota((2 * all_heads, width), 0), iota((2 * all_heads, width), 1)
        pick_b = jnp.where(pick_row == first + pick_col // HEAD, 1.0, 0.0).astype(BF16)
        pick_f = jnp.where(pick_row == all_heads + first + pick_col // HEAD, 1.0, 0.0).astype(BF16)
        spread = jnp.where(iota((heads, width), 0) == iota((heads, width), 1) // HEAD, 1.0, 0.0).astype(BF16)
        lane_head = iota((1, width), 1) // HEAD
        speed = jnp.zeros((1, width), F32)
        for h in range(heads):
            speed = jnp.where(lane_head == h, speed_ref[h], speed)
        rate = jnp.exp(speed)
        count = seqs * length // HEAD

        def prepare(n, carry):
            here = pl.ds(pl.multiple_of(n * HEAD, HEAD), HEAD)
            keys = silu(kv_acc[here, :width].astype(BF16).astype(F32))
            squares = keys * keys
            high = squares.astype(BF16)
            rest = (squares - high.astype(F32)).astype(BF16)
            norm = dot(high, mask) + dot(rest, mask)
            k_ref[here] = keys * lax.rsqrt(norm + 1e-06)
            v_ref[here] = silu(kv_acc[here, width:].astype(BF16).astype(F32))
            small = small_acc[here].astype(BF16)
            beta_ref[here] = 1.0 / (1.0 + jnp.exp(-dot(small, pick_b)))
            pre = dot(small, pick_f)
            soft = jnp.maximum(pre, 0.0) + jnp.log1p(jnp.exp(-jnp.abs(pre)))
            gamma = dot(extra_ref[here], spread) - rate * soft
            total_ref[here] = running_sum(gamma)
            return carry

        lax.fori_loop(0, count, prepare, 0)
        lane = iota((HEAD // 2, 128), 1)
        quarter_lane = iota((HEAD // 4, 128), 1)
        for s in range(seqs):
            parts = []
            for c in range(length // HEAD):
                here = pl.ds(s * length + c * HEAD, HEAD)
                parts.append(
                    chunk_map(k_ref[here], v_ref[here], beta_ref[here], total_ref[here], mask, heads)
                )
            removal, offset = composed(parts, lambda b, a: after(b, a, mask))
            for pair in range(heads // 2):
                r = removal[:, 128 * pair : 128 * (pair + 1)]
                o = offset[:, 128 * pair : 128 * (pair + 1)]
                top, bottom = r[: HEAD // 2], r[HEAD // 2 :]
                even = jnp.where(lane < HEAD, top, lanes_turned(bottom, HEAD))
                odd = jnp.where(lane < HEAD, lanes_turned(top, HEAD), bottom)
                for d in range(4):
                    dest = (s * heads + 2 * pair) * 2 + d
                    out_ref[dest, : HEAD // 2] = even if d < 2 else odd
                    packed = jnp.zeros((HEAD // 4, 128), F32)
                    for q in range(4):
                        piece = o[HEAD // 4 * q : HEAD // 4 * (q + 1)]
                        packed = jnp.where(quarter_lane // 32 == q, lanes_turned(piece, 32 * (q - d)), packed)
                    out_ref[dest, HEAD // 2 :] = packed


def owner_kernel(sources, q_ref, in_ref, out_ref, state_ref):
    lane = iota((HEAD, 128), 1)
    parts = []
    for i in range(sources):
        r, o = in_ref[i, : HEAD // 2], in_ref[i, HEAD // 2 :]
        left = jnp.concatenate([r, lanes_turned(r, HEAD)], axis=0)
        right = jnp.concatenate([lanes_turned(o, HEAD - 32 * q) for q in range(4)], axis=0)
        parts.append(jnp.where(lane < HEAD, left, jnp.where(lane < HEAD + 32, right, 0.0)))

    def combine(later, earlier):
        removal = jnp.where(lane < HEAD, later, 0.0)
        high = removal.astype(BF16)
        low = (removal - high.astype(F32)).astype(BF16)
        e_high = earlier.astype(BF16)
        e_low = (earlier - e_high.astype(F32)).astype(BF16)
        both = jnp.concatenate([e_high, e_high], axis=0)
        mixed = jnp.concatenate([e_low, e_low], axis=0)
        product = dot(high, both) + dot(high, mixed) + dot(low, both)
        return earlier + later - product

    final = composed(parts, combine)
    state_ref[...] = lanes_turned(final, HEAD)
    lane16 = iota((HEAD // 4, 128), 1)
    rows = jnp.zeros((HEAD // 4, 128), F32)
    for a in range(4):
        piece = state_ref[pl.ds(a, HEAD // 4, stride=4), :]
        rows = jnp.where(lane16 // 32 == a, lanes_turned(piece, 32 * a), rows)
    out_ref[:, :128] = rows
    state = state_ref[...]
    q = q_ref[...].astype(BF16)
    read = jnp.zeros((8, 128), F32)
    for _ in range(3):
        piece = state.astype(BF16)
        read = read + dot(q, piece)
        state = state - piece.astype(F32)
    out_ref[:, 128:] = jnp.broadcast_to(read[:1], (HEAD // 4, 128))


def body(
    layer_feed,
    address_mapping,
    content_mapping,
    beta_mapping_matrix,
    forgetting_mapping,
    logged_fading_speed,
    extra_forgetting,
    opening_probe,
):
    seqs, length, depth = layer_feed.shape
    width = address_mapping.shape[1]
    heads = width // HEAD
    all_heads = beta_mapping_matrix.shape[1]
    tokens = seqs * length
    ways = lax.axis_size("sp")
    steps = 8
    deep = depth // steps
    place = lax.axis_index("tp").astype(jnp.int32).reshape(1)
    whole = lambda i: (0, 0)
    maps = pl.pallas_call(
        functools.partial(local_kernel, heads, seqs, length),
        grid=(steps,),
        out_shape=jax.ShapeDtypeStruct((ways, 48, 128), F32),
        in_specs=[
            pl.BlockSpec(memory_space=pltpu.SMEM),
            pl.BlockSpec(memory_space=pltpu.SMEM),
            pl.BlockSpec((tokens, deep), lambda i: (0, i)),
            pl.BlockSpec((deep, width), lambda i: (i, 0)),
            pl.BlockSpec((deep, width), lambda i: (i, 0)),
            pl.BlockSpec((deep, all_heads), lambda i: (i, 0)),
            pl.BlockSpec((deep, all_heads), lambda i: (i, 0)),
            pl.BlockSpec((tokens, heads), whole),
        ],
        out_specs=pl.BlockSpec((ways, 48, 128), lambda i: (0, 0, 0)),
        scratch_shapes=[
            pltpu.VMEM((tokens, 2 * width), F32),
            pltpu.VMEM((tokens, 2 * all_heads), F32),
            pltpu.VMEM((width, width), BF16),
            pltpu.VMEM((tokens, width), F32),
            pltpu.VMEM((tokens, width), F32),
            pltpu.VMEM((tokens, width), F32),
            pltpu.VMEM((tokens, width), F32),
        ],
        compiler_params=pltpu.CompilerParams(vmem_limit_bytes=48 << 20),
        name="local_maps",
    )(
        place,
        logged_fading_speed,
        layer_feed.reshape(tokens, depth),
        address_mapping,
        content_mapping,
        beta_mapping_matrix,
        forgetting_mapping,
        extra_forgetting.reshape(tokens, heads),
    )
    got = lax.all_to_all(maps, "sp", 0, 0, tiled=True)
    group = lax.axis_index("sp") // 2
    query = lax.dynamic_slice_in_dim(opening_probe.reshape(seqs * heads, HEAD), group, 1, 0).astype(F32)
    query = jnp.pad(jnp.broadcast_to(query, (8, HEAD)), ((0, 0), (0, 0)))
    shares = pl.pallas_call(
        functools.partial(owner_kernel, ways),
        out_shape=jax.ShapeDtypeStruct((ways, 256), F32),
        scratch_shapes=[pltpu.VMEM((HEAD, 128), F32)],
        name="owner_state",
    )(query, got)
    mine = lax.all_to_all(shares.reshape(ways, 1, 256), "sp", 0, 0, tiled=True).reshape(ways, 256)
    rows = mine[:, :128].reshape(seqs * heads, 2, 4, 32).transpose(0, 2, 1, 3)
    context_memory_tensor = rows.reshape(seqs, heads, 4, HEAD).astype(BF16)
    read = mine[:, 128:160].reshape(seqs, heads, HEAD)
    read = read * lax.rsqrt(jnp.mean(read * read, axis=-1, keepdims=True) + 1e-06)
    return context_memory_tensor, read.reshape(seqs, width).astype(BF16)


def solution(mesh):
    in_specs = (
        P("grp", "sp", None),
        P(None, "tp"),
        P(None, "tp"),
        P(),
        P(),
        P("tp"),
        P("grp", "sp", "tp"),
        P("grp", "tp"),
    )
    out_specs = (P("grp", "tp", "sp", None), P("grp", "tp"))
    return jax.shard_map(body, mesh=mesh, in_specs=in_specs, out_specs=out_specs, check_vma=False)
```

```python
import functools

import jax
import jax.numpy as jnp
from jax import lax
from jax.experimental import pallas as pl
from jax.experimental.pallas import tpu as pltpu
from jax.sharding import PartitionSpec as P

HEAD = 64
BASE = 8
F32 = jnp.float32
BF16 = jnp.bfloat16


def iota(shape, dim):
    return lax.broadcasted_iota(jnp.int32, shape, dim)


def silu(v):
    return v / (1.0 + jnp.exp(-v))


def dot(a, b, dims=(1, 0)):
    return lax.dot_general(a, b, (((dims[0],), (dims[1],)), ((), ())), preferred_element_type=F32)


def lanes_turned(x, amount):
    amount %= x.shape[1]
    return pltpu.roll(x, amount, 1) if amount else x


def block_diagonal(x, mask):
    return jnp.tile(x, (mask.shape[0] // x.shape[0], 1)) * mask


def summed_from(x, direction):
    place = iota(x.shape, 1) % HEAD
    if direction < 0:
        place = HEAD - 1 - place
    step = 1
    while step < HEAD:
        x = x + jnp.where(place >= step, lanes_turned(x, direction * step), 0.0)
        step *= 2
    return x


def pieces_of(x, count):
    pieces = []
    for _ in range(count):
        piece = x.astype(BF16).astype(F32)
        pieces.append(piece)
        x = x - piece
    return pieces


def chunk_row(x, n, heads):
    here = x[:, 128 * (n // 2) : 128 * (n // 2 + 1)]
    turned = lanes_turned(here, HEAD)
    left, right = (here, turned) if n % 2 == 0 else (turned, here)
    first = iota((1, 128), 1) < HEAD
    return jnp.concatenate(
        [jnp.where(first, left[h : h + 1], right[h + 1 : h + 2]) for h in range(0, heads, 2)], axis=1
    )


def small_inverse(lower):
    width = lower.shape[1]
    block = iota((BASE, width), 1) % HEAD // BASE
    blocks = lower[:BASE]
    for r in range(1, HEAD // BASE):
        blocks = jnp.where(block == r, lower[BASE * r : BASE * (r + 1)], blocks)
    lane = iota((BASE, 128), 1)
    pieces = []
    for first in range(0, width, 128):
        part = blocks[:, first : first + 128]
        x = jnp.where(iota((BASE, 128), 0) == lane % BASE, 1.0, 0.0)
        for m in range(BASE - 1):
            factor = jnp.take_along_axis(part, lane // BASE * BASE + m, axis=1)
            x = x - factor * x[m : m + 1]
        pieces.append(x)
    inverse = jnp.concatenate(pieces, axis=1)
    return jnp.concatenate([jnp.where(block == r, inverse, 0.0) for r in range(HEAD // BASE)], axis=0)


def after(later, earlier, mask):
    high, low = pieces_of(later[0], 2)
    both = jnp.concatenate([high, low], axis=0).astype(BF16)
    joined = []
    for second, first in zip(later, earlier):
        first_high, first_low = pieces_of(first, 2)
        product = dot(both, block_diagonal(first_high.astype(BF16), mask))
        rest = dot(both[:HEAD], block_diagonal(first_low.astype(BF16), mask))
        joined.append(first + second - (product[:HEAD] + product[HEAD:] + rest))
    return tuple(joined)


def composed(parts, combine):
    while len(parts) > 1:
        joined = [combine(parts[i + 1], parts[i]) for i in range(0, len(parts) - 1, 2)]
        parts = joined + parts[len(joined) * 2 :]
    return parts[0]


def local_kernel(
    heads, place_ref, speed_ref, x_ref, wk_ref, wv_ref, wb_ref, wf_ref, extra_ref, out_ref,
    kv_acc, small_acc, wide_ref, k_ref, low_ref, taken_ref, added_ref, lower_ref, inverse_ref, inner_ref
):
    step = pl.program_id(0)
    width = heads * HEAD
    seqs, length, deep = x_ref.shape
    tokens = seqs * length
    all_heads = wb_ref.shape[0]

    @pl.when(step == 0)
    def _():
        kv_acc[...] = jnp.zeros_like(kv_acc)
        small_acc[...] = jnp.zeros_like(small_acc)

    x = x_ref[...].reshape(tokens, deep)
    kv_acc[:, :width] += dot(x, wk_ref[...])
    kv_acc[:, width:] += dot(x, wv_ref[...])
    small_acc[...] += dot(jnp.concatenate([wb_ref[...], wf_ref[...]], axis=0), x, (1, 1))

    @pl.when(step == pl.num_programs(0) - 1)
    def _():
        rows, cols = iota((width, width), 0), iota((width, width), 1)
        mask = jnp.where(rows // HEAD == cols // HEAD, 1.0, 0.0).astype(BF16)
        first = place_ref[0] * heads
        half = 2 * heads
        head_of_row = iota((half, 2 * all_heads), 0) % heads
        column = iota((half, 2 * all_heads), 1)
        small = small_acc[...].astype(BF16)
        beta_pre = dot(jnp.where(column == first + head_of_row, 1.0, 0.0).astype(BF16), small)
        decay_pre = dot(jnp.where(column == all_heads + first + head_of_row, 1.0, 0.0).astype(BF16), small)
        twice = jnp.where(iota((half, heads), 0) % heads == iota((half, heads), 1), 1.0, 0.0).astype(BF16)
        extra = jnp.concatenate([dot(twice, extra_ref[s]) for s in range(seqs)], axis=1)
        row_head = iota((half, 1), 0) % heads
        speed = jnp.zeros((half, 1), F32)
        for h in range(heads):
            speed = jnp.where(row_head == h, speed_ref[h], speed)
        soft = jnp.maximum(decay_pre, 0.0) + jnp.log1p(jnp.exp(-jnp.abs(decay_pre)))
        gamma = extra - jnp.exp(speed) * soft
        beta = 1.0 / (1.0 + jnp.exp(-beta_pre))
        total = summed_from(gamma, 1)
        last_lane = iota(gamma.shape, 1) % HEAD == HEAD - 1
        rest = summed_from(jnp.where(last_lane, 0.0, lanes_turned(gamma, -1)), -1)
        taking = beta * jnp.exp(total)
        carry = jnp.exp(rest)
        dropped = 1.0 - jnp.exp(total + rest)
        stack = pieces_of(beta, 2) + pieces_of(total, 3) + pieces_of(taking, 2)
        owner = [0] * 2 + [1] * 3 + [2] * 2
        pick_row, pick_col = iota((half * len(stack), 3 * width), 0), iota((half * len(stack), 3 * width), 1)
        kind = jnp.zeros(pick_row.shape, jnp.int32)
        for i, q in enumerate(owner):
            kind = jnp.where(pick_row // half == i, q, kind)
        pick = jnp.where((pick_col // width == kind) & (pick_row % half == pick_col % width // HEAD), 1.0, 0.0)
        wide_ref[...] = dot(jnp.concatenate(stack, axis=0).astype(BF16).T, pick.astype(BF16))

        count = tokens // HEAD
        for n in range(0, tokens, 256):
            here = pl.ds(n, 256)
            keys = silu(kv_acc[here, :width].astype(BF16).astype(F32))
            high, low = pieces_of(keys * keys, 2)
            norm = dot(high.astype(BF16), mask) + dot(low.astype(BF16), mask)
            keys = keys * lax.rsqrt(norm + 1e-06)
            k_ref[here] = keys
            low_ref[here] = keys.astype(BF16)
            taken_ref[here] = (keys * wide_ref[here, 2 * width :]).astype(BF16)
            values = silu(kv_acc[here, width:].astype(BF16).astype(F32))
            added_ref[here] = (values * wide_ref[here, :width]).astype(BF16)

        row, column = iota((HEAD, width), 0), iota((HEAD, width), 1) % HEAD
        for n in range(count):
            here = pl.ds(n * HEAD, HEAD)
            low = low_ref[here]
            gram = dot(low, block_diagonal(low, mask), (1, 1))
            gap = wide_ref[here, width : 2 * width] - chunk_row(total, n, heads)
            lower = wide_ref[here, :width] * gram * jnp.exp(jnp.minimum(gap, 0.0))
            lower = jnp.where(row > column, lower, 0.0)
            lower_ref[here] = lower.astype(BF16)
            inverse_ref[here] = small_inverse(lower)
        size = BASE
        while size < HEAD:
            level = (row // (2 * size) == column // (2 * size)) & (row // size > column // size)
            level = jnp.where(level, 1.0, 0.0).astype(BF16)
            for n in range(count):
                here = pl.ds(n * HEAD, HEAD)
                rounded = inverse_ref[here].astype(BF16)
                inner_ref[here] = dot(lower_ref[here] * level, block_diagonal(rounded, mask)).astype(BF16)
            for n in range(count):
                here = pl.ds(n * HEAD, HEAD)
                inverse = inverse_ref[here]
                inverse_ref[here] = inverse - dot(inverse.astype(BF16), block_diagonal(inner_ref[here], mask))
            size *= 2
        for n in range(count):
            here = pl.ds(n * HEAD, HEAD)
            turned = k_ref[here].T
            turned = jnp.concatenate([turned[HEAD * h : HEAD * (h + 1)] for h in range(heads)], axis=1)
            turned = (turned * chunk_row(carry, n, heads)).astype(BF16)
            inner_ref[here] = dot(turned, block_diagonal(inverse_ref[here].astype(BF16), mask)).astype(BF16)
        for n in range(count):
            here = pl.ds(n * HEAD, HEAD)
            closing = inner_ref[here]
            removal = dot(closing, block_diagonal(taken_ref[here], mask))
            k_ref[here] = removal + jnp.where(row == column, chunk_row(dropped, n, heads), 0.0)
            inverse_ref[here] = dot(closing, block_diagonal(added_ref[here], mask))
        span = length // HEAD
        reach = 1
        while reach < span:
            for s in range(seqs):
                for n in range(s * span, (s + 1) * span, 2 * reach):
                    low, high = pl.ds(n * HEAD, HEAD), pl.ds((n + reach) * HEAD, HEAD)
                    k_ref[low], inverse_ref[low] = after(
                        (k_ref[high], inverse_ref[high]), (k_ref[low], inverse_ref[low]), mask
                    )
            reach *= 2

        lane = iota((HEAD // 2, 128), 1)
        quarter_lane = iota((HEAD // 4, 128), 1)
        for s in range(seqs):
            here = pl.ds(s * length, HEAD)
            for pair in range(heads // 2):
                r = k_ref[here, 128 * pair : 128 * (pair + 1)]
                o = inverse_ref[here, 128 * pair : 128 * (pair + 1)]
                top, bottom = r[: HEAD // 2], r[HEAD // 2 :]
                even = jnp.where(lane < HEAD, top, lanes_turned(bottom, HEAD))
                odd = jnp.where(lane < HEAD, lanes_turned(top, HEAD), bottom)
                for d in range(4):
                    dest = (s * heads + 2 * pair) * 2 + d
                    out_ref[dest, : HEAD // 2] = even if d < 2 else odd
                    packed = jnp.zeros((HEAD // 4, 128), F32)
                    for q in range(4):
                        piece = o[HEAD // 4 * q : HEAD // 4 * (q + 1)]
                        packed = jnp.where(quarter_lane // 32 == q, lanes_turned(piece, 32 * (q - d)), packed)
                    out_ref[dest, HEAD // 2 :] = packed


def owner_kernel(sources, q_ref, in_ref, out_ref, state_ref):
    lane = iota((HEAD, 128), 1)
    parts = []
    for i in range(sources):
        r, o = in_ref[i, : HEAD // 2], in_ref[i, HEAD // 2 :]
        left = jnp.concatenate([r, lanes_turned(r, HEAD)], axis=0)
        right = jnp.concatenate([lanes_turned(o, HEAD - 32 * q) for q in range(4)], axis=0)
        parts.append(jnp.where(lane < HEAD, left, jnp.where(lane < HEAD + 32, right, 0.0)))

    def combine(later, earlier):
        high, low = pieces_of(jnp.where(lane < HEAD, later, 0.0), 2)
        first_high, first_low = pieces_of(earlier, 2)
        left = jnp.concatenate([high + lanes_turned(low, HEAD), high], axis=1).astype(BF16)
        right = jnp.concatenate([first_high, first_high, first_low, first_low], axis=0).astype(BF16)
        return earlier + later - dot(left, right)

    final = composed(parts, combine)
    state_ref[...] = lanes_turned(final, HEAD)
    lane16 = iota((HEAD // 4, 128), 1)
    rows = jnp.zeros((HEAD // 4, 128), F32)
    for a in range(4):
        piece = state_ref[pl.ds(a, HEAD // 4, stride=4), :]
        rows = jnp.where(lane16 // 32 == a, lanes_turned(piece, 32 * a), rows)
    out_ref[:, :128] = rows
    state = state_ref[...]
    q = q_ref[...].astype(BF16)
    read = jnp.zeros((8, 128), F32)
    for _ in range(3):
        piece = state.astype(BF16)
        read = read + dot(q, piece)
        state = state - piece.astype(F32)
    out_ref[:, 128:] = jnp.broadcast_to(read[:1], (HEAD // 4, 128))


def body(
    layer_feed,
    address_mapping,
    content_mapping,
    beta_mapping_matrix,
    forgetting_mapping,
    logged_fading_speed,
    extra_forgetting,
    opening_probe,
):
    seqs, length, depth = layer_feed.shape
    width = address_mapping.shape[1]
    heads = width // HEAD
    all_heads = beta_mapping_matrix.shape[1]
    tokens = seqs * length
    ways = lax.axis_size("sp")
    steps = 4
    deep = depth // steps
    place = lax.axis_index("tp").astype(jnp.int32).reshape(1)
    share = (ways, 3 * HEAD // 4, 128)
    maps = pl.pallas_call(
        functools.partial(local_kernel, heads),
        grid=(steps,),
        out_shape=jax.ShapeDtypeStruct(share, F32),
        in_specs=[
            pl.BlockSpec(memory_space=pltpu.SMEM),
            pl.BlockSpec(memory_space=pltpu.SMEM),
            pl.BlockSpec((seqs, length, deep), lambda i: (0, 0, i)),
            pl.BlockSpec((deep, width), lambda i: (i, 0)),
            pl.BlockSpec((deep, width), lambda i: (i, 0)),
            pl.BlockSpec((all_heads, deep), lambda i: (0, i)),
            pl.BlockSpec((all_heads, deep), lambda i: (0, i)),
            pl.BlockSpec((seqs, heads, length), lambda i: (0, 0, 0)),
        ],
        out_specs=pl.BlockSpec(share, lambda i: (0, 0, 0)),
        scratch_shapes=[
            pltpu.VMEM((tokens, 2 * width), F32),
            pltpu.VMEM((2 * all_heads, tokens), F32),
            pltpu.VMEM((tokens, 3 * width), F32),
            pltpu.VMEM((tokens, width), F32),
            pltpu.VMEM((tokens, width), BF16),
            pltpu.VMEM((tokens, width), BF16),
            pltpu.VMEM((tokens, width), BF16),
            pltpu.VMEM((tokens, width), BF16),
            pltpu.VMEM((tokens, width), F32),
            pltpu.VMEM((tokens, width), BF16),
        ],
        compiler_params=pltpu.CompilerParams(vmem_limit_bytes=63 << 20),
        name="local_maps",
    )(
        place,
        logged_fading_speed,
        layer_feed,
        address_mapping,
        content_mapping,
        beta_mapping_matrix.T,
        forgetting_mapping.T,
        extra_forgetting.transpose(0, 2, 1),
    )
    got = lax.all_to_all(maps, "sp", 0, 0, tiled=True)
    group = lax.axis_index("sp") // 2
    query = lax.dynamic_slice_in_dim(opening_probe.reshape(seqs * heads, HEAD), group, 1, 0).astype(F32)
    query = jnp.broadcast_to(query, (8, HEAD))
    shares = pl.pallas_call(
        functools.partial(owner_kernel, ways),
        out_shape=jax.ShapeDtypeStruct((ways, 256), F32),
        scratch_shapes=[pltpu.VMEM((HEAD, 128), F32)],
        name="owner_state",
    )(query, got)
    mine = lax.all_to_all(shares.reshape(ways, 1, 256), "sp", 0, 0, tiled=True).reshape(ways, 256)
    rows = mine[:, :128].reshape(seqs * heads, 2, 4, 32).transpose(0, 2, 1, 3)
    context_memory_tensor = rows.reshape(seqs, heads, 4, HEAD).astype(BF16)
    read = mine[:, 128:160].reshape(seqs, heads, HEAD)
    read = read * lax.rsqrt(jnp.mean(read * read, axis=-1, keepdims=True) + 1e-06)
    return context_memory_tensor, read.reshape(seqs, width).astype(BF16)


def solution(mesh):
    in_specs = (
        P("grp", "sp", None),
        P(None, "tp"),
        P(None, "tp"),
        P(),
        P(),
        P("tp"),
        P("grp", "sp", "tp"),
        P("grp", "tp"),
    )
    out_specs = (P("grp", "tp", "sp", None), P("grp", "tp"))
    return jax.shard_map(body, mesh=mesh, in_specs=in_specs, out_specs=out_specs, check_vma=False)
```

```python
import functools

import jax
import jax.numpy as jnp
from jax import lax
from jax.experimental import pallas as pl
from jax.experimental.pallas import tpu as pltpu
from jax.sharding import PartitionSpec as P

HEAD = 64
BASE = 8
F32 = jnp.float32
BF16 = jnp.bfloat16


def iota(shape, dim):
    return lax.broadcasted_iota(jnp.int32, shape, dim)


def silu(v):
    return v / (1.0 + jnp.exp(-v))


def dot(a, b, dims=(1, 0)):
    return lax.dot_general(a, b, (((dims[0],), (dims[1],)), ((), ())), preferred_element_type=F32)


def lanes_turned(x, amount):
    amount %= x.shape[1]
    return pltpu.roll(x, amount, 1) if amount else x


def split(x):
    high = x.astype(BF16)
    return high, (x - high.astype(F32)).astype(BF16)


def block_diagonal(x, lane_masks):
    heads = x.shape[1] // HEAD
    empty = jnp.zeros((x.shape[0], 128), x.dtype)
    rows = []
    for h in range(heads):
        pair = h // 2
        own = x[:, 128 * pair : 128 * (pair + 1)] * lane_masks[h % 2]
        rows.append(jnp.concatenate([own if p == pair else empty for p in range(heads // 2)], axis=1))
    return jnp.concatenate(rows, axis=0)


def pair_diagonal(x, lane_masks):
    tiles = [x[:, f : f + 128] for f in range(0, x.shape[1], 128)]
    return jnp.concatenate(
        [jnp.concatenate([t * lane_masks[h] for t in tiles], axis=1) for h in range(2)], axis=0
    )


def chunk_row(x, n, heads):
    here = x[:, 128 * (n // 2) : 128 * (n // 2 + 1)]
    turned = lanes_turned(here, HEAD)
    left, right = (here, turned) if n % 2 == 0 else (turned, here)
    first = iota((1, 128), 1) < HEAD
    return jnp.concatenate(
        [jnp.where(first, left[h : h + 1], right[h + 1 : h + 2]) for h in range(0, heads, 2)], axis=1
    )


def left_after(x):
    size = x.shape[1]
    place = iota(x.shape, 1)
    x = jnp.where(place < size - 1, lanes_turned(x, -1), 0.0)
    step = 1
    while step < size:
        x = x + jnp.where(place < size - step, lanes_turned(x, -step), 0.0)
        step *= 2
    return x


def diagonal_blocks(x):
    block = iota((BASE, x.shape[1]), 1) % HEAD // BASE
    blocks = x[:BASE]
    for r in range(1, HEAD // BASE):
        blocks = jnp.where(block == r, x[BASE * r : BASE * (r + 1)], blocks)
    return blocks


def composed(parts, combine):
    while len(parts) > 1:
        joined = [combine(parts[i + 1], parts[i]) for i in range(0, len(parts) - 1, 2)]
        parts = joined + parts[len(joined) * 2 :]
    return parts[0]


def local_kernel(
    heads, place_ref, speed_ref, x_ref, wk_ref, wv_ref, wb_ref, wf_ref, extra_ref, out_ref,
    kv_acc, small_acc, wide_ref, turned_ref, key_ref, lower_ref, inverse_ref, inner_ref, map_ref,
    blocks_ref, factor_ref
):
    step = pl.program_id(0)
    width = heads * HEAD
    seqs, length, deep = x_ref.shape
    tokens = seqs * length
    all_heads = wb_ref.shape[0]

    @pl.when(step == 0)
    def _():
        kv_acc[...] = jnp.zeros_like(kv_acc)
        small_acc[...] = jnp.zeros_like(small_acc)

    x = x_ref[...].reshape(tokens, deep)
    kv_acc[:, :width] += dot(x, wk_ref[...])
    kv_acc[:, width:] += dot(x, wv_ref[...])
    small_acc[...] += dot(jnp.concatenate([wb_ref[...], wf_ref[...]], axis=0), x, (1, 1))

    @pl.when(step == pl.num_programs(0) - 1)
    def _():
        first = place_ref[0] * heads
        half = 2 * heads
        head_of_row = iota((half, 2 * all_heads), 0) % heads
        column = iota((half, 2 * all_heads), 1)
        small = small_acc[...].astype(BF16)
        beta_pre = dot(jnp.where(column == first + head_of_row, 1.0, 0.0).astype(BF16), small)
        decay_pre = dot(jnp.where(column == all_heads + first + head_of_row, 1.0, 0.0).astype(BF16), small)
        twice = jnp.where(iota((half, heads), 0) % heads == iota((half, heads), 1), 1.0, 0.0).astype(BF16)
        row_head = iota((half, 1), 0) % heads
        speed = jnp.zeros((half, 1), F32)
        for h in range(heads):
            speed = jnp.where(row_head == h, speed_ref[h], speed)
        rate = jnp.exp(speed)
        soft = jnp.maximum(decay_pre, 0.0) + jnp.log1p(jnp.exp(-jnp.abs(decay_pre)))
        beta = 1.0 / (1.0 + jnp.exp(-beta_pre))
        decays, kept = [], []
        for s in range(seqs):
            gamma = dot(twice, extra_ref[s]) - rate * soft[:, s * length : (s + 1) * length]
            behind = left_after(gamma)
            decays.append(jnp.exp(behind))
            kept.append(jnp.exp(gamma[:, :1] + behind[:, :1]))
        stack = jnp.concatenate([p.astype(F32) for p in split(jnp.concatenate(decays, axis=1))], axis=0)
        pick = iota((2 * half, width), 0) % half == iota((2 * half, width), 1) // HEAD
        wide_ref[...] = dot(stack.T.astype(BF16), jnp.where(pick, 1.0, 0.0).astype(BF16))

        low_lanes = iota((HEAD, 128), 1) < HEAD
        lane_masks = [jnp.where(low_lanes, 1.0, 0.0).astype(BF16), jnp.where(low_lanes, 0.0, 1.0).astype(BF16)]
        same_head = iota((width, width), 0) // HEAD == iota((width, width), 1) // HEAD
        ones = jnp.where(same_head, 1.0, 0.0).astype(BF16)
        count = tokens // HEAD
        span = length // HEAD
        chunks = [pl.ds(n * HEAD, HEAD) for n in range(count)]
        for n in range(0, count, 2):
            here = pl.ds(n * HEAD, 2 * HEAD)
            keys = silu(kv_acc[here, :width].astype(BF16).astype(F32))
            norm = dot((keys * keys).astype(BF16), ones)
            keys = keys * lax.rsqrt(norm + 1e-06)
            key_ref[here] = keys.astype(BF16)
            turned = keys.astype(BF16).T
            for c in range(2):
                turned_ref[chunks[n + c]] = jnp.concatenate(
                    [turned[HEAD * h : HEAD * (h + 1), HEAD * c : HEAD * (c + 1)] for h in range(heads)], axis=1
                )
        row, column = iota((HEAD, width), 0), iota((HEAD, width), 1) % HEAD
        for n, here in enumerate(chunks):
            lower = dot(key_ref[here], block_diagonal(turned_ref[here], lane_masks))
            lower = jnp.where(row > column, lower * chunk_row(beta, n, heads), 0.0)
            lower_ref[here] = lower.astype(BF16)
            blocks = diagonal_blocks(lower)
            for f in range(0, width, 128):
                blocks_ref[pl.ds((n * width + f) // 128 * BASE, BASE)] = blocks[:, f : f + 128]
        spread_row, spread_col = iota((128, 128), 0), iota((128, 128), 1)
        spread = jnp.concatenate(
            [
                jnp.where(spread_row == spread_col // BASE * BASE + m, 1.0, 0.0).astype(BF16)
                for m in range(BASE - 1)
            ],
            axis=1,
        )
        factor_ref[...] = dot(blocks_ref[...].astype(BF16), spread)
        sets = blocks_ref.shape[0] // BASE
        solved = jnp.where(iota((BASE, 128), 0) == iota((BASE, 128), 1) % BASE, 1.0, 0.0)
        solved = jnp.broadcast_to(solved[None], (sets, BASE, 128))
        for m in range(BASE - 1):
            factor = factor_ref[:, 128 * m : 128 * (m + 1)].reshape(sets, BASE, 128)
            solved = solved - factor * solved[:, m : m + 1]
        blocks_ref[...] = solved.reshape(sets * BASE, 128)
        block = iota((BASE, width), 1) % HEAD // BASE
        for n, here in enumerate(chunks):
            own = jnp.concatenate(
                [blocks_ref[pl.ds((n * width + f) // 128 * BASE, BASE)] for f in range(0, width, 128)], axis=1
            )
            inverse_ref[here] = jnp.concatenate(
                [jnp.where(block == r, own, 0.0) for r in range(HEAD // BASE)], axis=0
            )
        level = (row // (2 * BASE) == column // (2 * BASE)) & (row // BASE > column // BASE)
        level = jnp.where(level, 1.0, 0.0).astype(BF16)
        for here in chunks:
            rounded = block_diagonal(inverse_ref[here].astype(BF16), lane_masks)
            inner_ref[here] = dot(lower_ref[here] * level, rounded).astype(BF16)
        for here in chunks:
            inverse = inverse_ref[here]
            inner = block_diagonal(inner_ref[here], lane_masks)
            inverse_ref[here] = inverse - dot(inverse.astype(BF16), inner)
        size = 2 * BASE
        while size < HEAD:
            odd = range(size, HEAD, 2 * size)
            block = iota((size, width), 1) % HEAD // size
            gap = jnp.zeros((size, width), BF16)
            for n in range(count):
                rounded = block_diagonal(inverse_ref[chunks[n]].astype(BF16), lane_masks)
                off = [
                    jnp.where(block == r // size - 1, lower_ref[pl.ds(n * HEAD + r, size)], gap) for r in odd
                ]
                inner_ref[pl.ds(n * HEAD, HEAD // 2)] = dot(jnp.concatenate(off, axis=0), rounded).astype(BF16)
            for n in range(count):
                inner = []
                for i, r in enumerate(odd):
                    inner += [gap, inner_ref[pl.ds(n * HEAD + i * size, size)]]
                inner = block_diagonal(jnp.concatenate(inner, axis=0), lane_masks)
                places = [pl.ds(n * HEAD + r, size) for r in odd]
                inverse = jnp.concatenate([inverse_ref[p] for p in places], axis=0)
                inverse = inverse - dot(inverse.astype(BF16), inner)
                for i, p in enumerate(places):
                    inverse_ref[p] = inverse[i * size : (i + 1) * size]
            size *= 2
        for n, here in enumerate(chunks):
            inverse = block_diagonal(inverse_ref[here].astype(BF16), lane_masks)
            turned = (turned_ref[here].astype(F32) * chunk_row(beta, n, heads)).astype(BF16)
            inner_ref[here] = dot(turned, inverse).astype(BF16)
        for here in chunks:
            added = (silu(kv_acc[here, width:].astype(BF16).astype(F32)) * wide_ref[here]).astype(BF16)
            for f in range(0, width, 128):
                both = jnp.concatenate([key_ref[here, f : f + 128], added[:, f : f + 128]], axis=1)
                map_ref[here, 2 * f : 2 * f + 256] = dot(inner_ref[here, f : f + 128], pair_diagonal(both, lane_masks))
        reach = 1
        while reach < span:
            for n in range(0, count, 2 * reach):
                early, late = chunks[n], chunks[n + reach]
                for f in range(0, 2 * width, 256):
                    before, later = map_ref[early, f : f + 256], map_ref[late, f : f + 256]
                    carried = dot(later[:, :128].astype(BF16), pair_diagonal(before.astype(BF16), lane_masks))
                    map_ref[early, f : f + 256] = before + later - carried
            reach *= 2

        lane = iota((HEAD // 2, 128), 1)
        quarter_lane = iota((HEAD // 4, 128), 1)
        lane_head = iota((1, width), 1) // HEAD
        for s in range(seqs):
            here = chunks[s * span]
            keep = jnp.zeros((1, width), F32)
            for h in range(heads):
                keep = jnp.where(lane_head == h, kept[s][h : h + 1], keep)
            for pair in range(heads // 2):
                part = slice(128 * pair, 128 * (pair + 1))
                r = keep[:, part] * map_ref[here, 256 * pair : 256 * pair + 128]
                r = r + jnp.where(row[:, part] == column[:, part], 1.0 - keep[:, part], 0.0)
                o = map_ref[here, 256 * pair + 128 : 256 * (pair + 1)]
                top, bottom = r[: HEAD // 2], r[HEAD // 2 :]
                even = jnp.where(lane < HEAD, top, lanes_turned(bottom, HEAD))
                odd = jnp.where(lane < HEAD, lanes_turned(top, HEAD), bottom)
                for d in range(4):
                    dest = (s * heads + 2 * pair) * 2 + d
                    out_ref[dest, : HEAD // 2] = even if d < 2 else odd
                    packed = jnp.zeros((HEAD // 4, 128), F32)
                    for q in range(4):
                        piece = o[HEAD // 4 * q : HEAD // 4 * (q + 1)]
                        packed = jnp.where(quarter_lane // 32 == q, lanes_turned(piece, 32 * (q - d)), packed)
                    out_ref[dest, HEAD // 2 :] = packed


def owner_kernel(heads, place_ref, probe_ref, in_ref, out_ref):
    sources = in_ref.shape[0]
    lane = iota((HEAD, 128), 1)
    parts = []
    for i in range(sources):
        r, o = in_ref[i, : HEAD // 2], in_ref[i, HEAD // 2 :]
        left = jnp.concatenate([r, lanes_turned(r, HEAD)], axis=0)
        right = jnp.concatenate([lanes_turned(o, HEAD - 32 * q) for q in range(4)], axis=0)
        parts.append(jnp.where(lane < HEAD, left, jnp.where(lane < HEAD + 32, right, 0.0)))

    def combine(later, earlier):
        removal = jnp.where(lane < HEAD, later, 0.0)
        high = removal.astype(BF16)
        low = lanes_turned(removal - high.astype(F32), HEAD).astype(BF16)
        first_high, first_low = split(earlier)
        left = jnp.concatenate([high + low, high], axis=1)
        right = jnp.concatenate([first_high, first_high, first_low, first_low], axis=0)
        return earlier + later - dot(left, right)

    state = lanes_turned(composed(parts, combine), HEAD)
    share = HEAD // sources
    for j in range(sources):
        out_ref[j, :share] = state[share * j : share * (j + 1)]
    group = place_ref[0] // 2
    probe = probe_ref[...].astype(F32)
    probe = jnp.where(iota(probe.shape, 0) == group // heads, probe, 0.0)
    probe = jnp.sum(probe, axis=0, keepdims=True)
    query = jnp.zeros((1, 128), F32)
    for h in range(heads):
        pair = probe[:, 128 * (h // 2) : 128 * (h // 2 + 1)]
        query = jnp.where(group % heads == h, lanes_turned(pair, HEAD) if h % 2 else pair, query)
    query = jnp.broadcast_to(query[:, :HEAD], (8, HEAD)).astype(BF16)
    read = jnp.zeros((8, 128), F32)
    for _ in range(3):
        piece = state.astype(BF16)
        read = read + dot(query, piece)
        state = state - piece.astype(F32)
    for j in range(sources):
        out_ref[j, share:] = read[share:]


def result_kernel(in_ref, rows_ref, read_ref):
    seqs, heads, share, _ = rows_ref.shape
    lane = iota((8, 128), 1)
    reads = []
    for g in range(seqs * heads):
        both = jnp.where(lane < HEAD // 2, in_ref[2 * g], lanes_turned(in_ref[2 * g + 1], HEAD // 2))
        rows_ref[g // heads, g % heads] = both[:share, :HEAD].astype(BF16)
        read = jnp.where(lane < HEAD, both, 0.0)[share : share + 1]
        mean = jnp.sum(read * read, axis=1, keepdims=True) / HEAD
        reads.append(read * lax.rsqrt(mean + 1e-06))
    for s in range(seqs):
        own = reads[s * heads : (s + 1) * heads]
        pairs = [own[h] + lanes_turned(own[h + 1], HEAD) for h in range(0, heads, 2)]
        read_ref[pl.ds(s, 1)] = jnp.concatenate(pairs, axis=1).astype(BF16)


def body(
    layer_feed,
    address_mapping,
    content_mapping,
    beta_mapping_matrix,
    forgetting_mapping,
    logged_fading_speed,
    extra_forgetting,
    opening_probe,
):
    seqs, length, depth = layer_feed.shape
    width = address_mapping.shape[1]
    heads = width // HEAD
    all_heads = beta_mapping_matrix.shape[1]
    tokens = seqs * length
    ways = lax.axis_size("sp")
    steps = 4
    deep = depth // steps
    place = lax.axis_index("tp").astype(jnp.int32).reshape(1)
    share = (ways, 3 * HEAD // 4, 128)
    maps = pl.pallas_call(
        functools.partial(local_kernel, heads),
        grid=(steps,),
        out_shape=jax.ShapeDtypeStruct(share, F32),
        in_specs=[
            pl.BlockSpec(memory_space=pltpu.SMEM),
            pl.BlockSpec(memory_space=pltpu.SMEM),
            pl.BlockSpec((seqs, length, deep), lambda i: (0, 0, i)),
            pl.BlockSpec((deep, width), lambda i: (i, 0)),
            pl.BlockSpec((deep, width), lambda i: (i, 0)),
            pl.BlockSpec((all_heads, deep), lambda i: (0, i)),
            pl.BlockSpec((all_heads, deep), lambda i: (0, i)),
            pl.BlockSpec((seqs, heads, length), lambda i: (0, 0, 0)),
        ],
        out_specs=pl.BlockSpec(share, lambda i: (0, 0, 0)),
        scratch_shapes=[
            pltpu.VMEM((tokens, 2 * width), F32),
            pltpu.VMEM((2 * all_heads, tokens), F32),
            pltpu.VMEM((tokens, width), F32),
            pltpu.VMEM((tokens, width), BF16),
            pltpu.VMEM((tokens, width), BF16),
            pltpu.VMEM((tokens, width), BF16),
            pltpu.VMEM((tokens, width), F32),
            pltpu.VMEM((tokens, width), BF16),
            pltpu.VMEM((tokens, 2 * width), F32),
            pltpu.VMEM((tokens * width // HEAD // 128 * BASE, 128), F32),
            pltpu.VMEM((tokens * width // HEAD // 128 * BASE, 128 * (BASE - 1)), F32),
        ],
        compiler_params=pltpu.CompilerParams(vmem_limit_bytes=63 << 20),
        name="local_maps",
    )(
        place,
        logged_fading_speed,
        layer_feed,
        address_mapping,
        content_mapping,
        beta_mapping_matrix.T,
        forgetting_mapping.T,
        extra_forgetting.transpose(0, 2, 1),
    )
    got = lax.all_to_all(maps, "sp", 0, 0, tiled=True)
    turn = lax.axis_index("sp").astype(jnp.int32).reshape(1)
    shares = pl.pallas_call(
        functools.partial(owner_kernel, heads),
        out_shape=jax.ShapeDtypeStruct((ways, 8, 128), F32),
        in_specs=[
            pl.BlockSpec(memory_space=pltpu.SMEM),
            pl.BlockSpec(memory_space=pltpu.VMEM),
            pl.BlockSpec(memory_space=pltpu.VMEM),
        ],
        compiler_params=pltpu.CompilerParams(vmem_limit_bytes=8 << 20),
        name="owner_state",
    )(turn, opening_probe, got)
    mine = lax.all_to_all(shares, "sp", 0, 0, tiled=True)
    return pl.pallas_call(
        result_kernel,
        out_shape=(
            jax.ShapeDtypeStruct((seqs, heads, HEAD // ways, HEAD), BF16),
            jax.ShapeDtypeStruct((seqs, width), BF16),
        ),
        compiler_params=pltpu.CompilerParams(vmem_limit_bytes=8 << 20),
        name="results",
    )(mine)


def solution(mesh):
    in_specs = (
        P("grp", "sp", None),
        P(None, "tp"),
        P(None, "tp"),
        P(),
        P(),
        P("tp"),
        P("grp", "sp", "tp"),
        P("grp", "tp"),
    )
    out_specs = (P("grp", "tp", "sp", None), P("grp", "tp"))
    return jax.shard_map(body, mesh=mesh, in_specs=in_specs, out_specs=out_specs, check_vma=False)
```

```python
import functools

import jax
import jax.numpy as jnp
from jax import lax
from jax.experimental import pallas as pl
from jax.experimental.pallas import tpu as pltpu
from jax.sharding import PartitionSpec as P

HEAD = 64
BASE = 8
F32 = jnp.float32
BF16 = jnp.bfloat16


def iota(shape, dim):
    return lax.broadcasted_iota(jnp.int32, shape, dim)


def silu(v):
    return v / (1.0 + jnp.exp(-v))


def dot(a, b, dims=(1, 0)):
    return lax.dot_general(a, b, (((dims[0],), (dims[1],)), ((), ())), preferred_element_type=F32)


def lanes_turned(x, amount):
    amount %= x.shape[1]
    return pltpu.roll(x, amount, 1) if amount else x


def split(x):
    high = x.astype(BF16)
    return high, (x - high.astype(F32)).astype(BF16)


def block_diagonal(x, lane_masks):
    heads = x.shape[1] // HEAD
    empty = jnp.zeros((x.shape[0], 128), x.dtype)
    rows = []
    for h in range(heads):
        pair = h // 2
        own = x[:, 128 * pair : 128 * (pair + 1)] * lane_masks[h % 2]
        rows.append(jnp.concatenate([own if p == pair else empty for p in range(heads // 2)], axis=1))
    return jnp.concatenate(rows, axis=0)


def pair_diagonal(x, lane_masks):
    tiles = [x[:, f : f + 128] for f in range(0, x.shape[1], 128)]
    return jnp.concatenate(
        [jnp.concatenate([t * lane_masks[h] for t in tiles], axis=1) for h in range(2)], axis=0
    )


def chunk_row(x, n, heads):
    here = x[:, 128 * (n // 2) : 128 * (n // 2 + 1)]
    turned = lanes_turned(here, HEAD)
    left, right = (here, turned) if n % 2 == 0 else (turned, here)
    first = iota((1, 128), 1) < HEAD
    return jnp.concatenate(
        [jnp.where(first, left[h : h + 1], right[h + 1 : h + 2]) for h in range(0, heads, 2)], axis=1
    )


def left_after(x):
    size = x.shape[1]
    place = iota(x.shape, 1)
    x = jnp.where(place < size - 1, lanes_turned(x, -1), 0.0)
    step = 1
    while step < size:
        x = x + jnp.where(place < size - step, lanes_turned(x, -step), 0.0)
        step *= 2
    return x


def diagonal_blocks(x):
    block = iota((BASE, x.shape[1]), 1) % HEAD // BASE
    blocks = x[:BASE]
    for r in range(1, HEAD // BASE):
        blocks = jnp.where(block == r, x[BASE * r : BASE * (r + 1)], blocks)
    return blocks


def composed(parts, combine):
    while len(parts) > 1:
        joined = [combine(parts[i + 1], parts[i]) for i in range(0, len(parts) - 1, 2)]
        parts = joined + parts[len(joined) * 2 :]
    return parts[0]


def local_kernel(
    heads, place_ref, speed_ref, x_ref, wk_ref, wv_ref, wb_ref, wf_ref, extra_ref, kept_ref, sent_ref,
    kv_acc, small_acc, wide_ref, turned_ref, key_ref, lower_ref, inverse_ref, inner_ref, map_ref,
    blocks_ref, factor_ref
):
    step = pl.program_id(0)
    width = heads * HEAD
    seqs, length, deep = x_ref.shape
    tokens = seqs * length
    all_heads = wb_ref.shape[0]

    @pl.when(step == 0)
    def _():
        kv_acc[...] = jnp.zeros_like(kv_acc)
        small_acc[...] = jnp.zeros_like(small_acc)

    x = x_ref[...].reshape(tokens, deep)
    kv_acc[:, :width] += dot(x, wk_ref[...])
    kv_acc[:, width:] += dot(x, wv_ref[...])
    small_acc[...] += dot(jnp.concatenate([wb_ref[...], wf_ref[...]], axis=0), x, (1, 1))

    @pl.when(step == pl.num_programs(0) - 1)
    def _():
        first = place_ref[0] * heads
        half = 2 * heads
        head_of_row = iota((half, 2 * all_heads), 0) % heads
        column = iota((half, 2 * all_heads), 1)
        small = small_acc[...].astype(BF16)
        beta_pre = dot(jnp.where(column == first + head_of_row, 1.0, 0.0).astype(BF16), small)
        decay_pre = dot(jnp.where(column == all_heads + first + head_of_row, 1.0, 0.0).astype(BF16), small)
        twice = jnp.where(iota((half, heads), 0) % heads == iota((half, heads), 1), 1.0, 0.0).astype(BF16)
        row_head = iota((half, 1), 0) % heads
        speed = jnp.zeros((half, 1), F32)
        for h in range(heads):
            speed = jnp.where(row_head == h, speed_ref[h], speed)
        rate = jnp.exp(speed)
        soft = jnp.maximum(decay_pre, 0.0) + jnp.log1p(jnp.exp(-jnp.abs(decay_pre)))
        beta = 1.0 / (1.0 + jnp.exp(-beta_pre))
        decays, kept = [], []
        for s in range(seqs):
            gamma = dot(twice, extra_ref[s]) - rate * soft[:, s * length : (s + 1) * length]
            behind = left_after(gamma)
            decays.append(jnp.exp(behind))
            kept.append(jnp.exp(gamma[:, :1] + behind[:, :1]))
        stack = jnp.concatenate([p.astype(F32) for p in split(jnp.concatenate(decays, axis=1))], axis=0)
        pick = iota((2 * half, width), 0) % half == iota((2 * half, width), 1) // HEAD
        wide_ref[...] = dot(stack.T.astype(BF16), jnp.where(pick, 1.0, 0.0).astype(BF16))

        low_lanes = iota((HEAD, 128), 1) < HEAD
        lane_masks = [jnp.where(low_lanes, 1.0, 0.0).astype(BF16), jnp.where(low_lanes, 0.0, 1.0).astype(BF16)]
        same_head = iota((width, width), 0) // HEAD == iota((width, width), 1) // HEAD
        ones = jnp.where(same_head, 1.0, 0.0).astype(BF16)
        count = tokens // HEAD
        span = length // HEAD
        chunks = [pl.ds(n * HEAD, HEAD) for n in range(count)]
        for n in range(0, count, 2):
            here = pl.ds(n * HEAD, 2 * HEAD)
            keys = silu(kv_acc[here, :width].astype(BF16).astype(F32))
            norm = dot((keys * keys).astype(BF16), ones)
            keys = keys * lax.rsqrt(norm + 1e-06)
            key_ref[here] = keys.astype(BF16)
            turned = keys.astype(BF16).T
            for c in range(2):
                turned_ref[chunks[n + c]] = jnp.concatenate(
                    [turned[HEAD * h : HEAD * (h + 1), HEAD * c : HEAD * (c + 1)] for h in range(heads)], axis=1
                )
        row, column = iota((HEAD, width), 0), iota((HEAD, width), 1) % HEAD
        for n, here in enumerate(chunks):
            lower = dot(key_ref[here], block_diagonal(turned_ref[here], lane_masks))
            lower = jnp.where(row > column, lower * chunk_row(beta, n, heads), 0.0)
            lower_ref[here] = lower.astype(BF16)
            blocks = diagonal_blocks(lower)
            for f in range(0, width, 128):
                blocks_ref[pl.ds((n * width + f) // 128 * BASE, BASE)] = blocks[:, f : f + 128]
        spread_row, spread_col = iota((128, 128), 0), iota((128, 128), 1)
        spread = jnp.concatenate(
            [
                jnp.where(spread_row == spread_col // BASE * BASE + m, 1.0, 0.0).astype(BF16)
                for m in range(BASE - 1)
            ],
            axis=1,
        )
        factor_ref[...] = dot(blocks_ref[...].astype(BF16), spread)
        sets = blocks_ref.shape[0] // BASE
        solved = jnp.where(iota((BASE, 128), 0) == iota((BASE, 128), 1) % BASE, 1.0, 0.0)
        solved = jnp.broadcast_to(solved[None], (sets, BASE, 128))
        for m in range(BASE - 1):
            factor = factor_ref[:, 128 * m : 128 * (m + 1)].reshape(sets, BASE, 128)
            solved = solved - factor * solved[:, m : m + 1]
        blocks_ref[...] = solved.reshape(sets * BASE, 128)
        block = iota((BASE, width), 1) % HEAD // BASE
        for n, here in enumerate(chunks):
            own = jnp.concatenate(
                [blocks_ref[pl.ds((n * width + f) // 128 * BASE, BASE)] for f in range(0, width, 128)], axis=1
            )
            inverse_ref[here] = jnp.concatenate(
                [jnp.where(block == r, own, 0.0) for r in range(HEAD // BASE)], axis=0
            )
        level = (row // (2 * BASE) == column // (2 * BASE)) & (row // BASE > column // BASE)
        level = jnp.where(level, 1.0, 0.0).astype(BF16)
        for here in chunks:
            rounded = block_diagonal(inverse_ref[here].astype(BF16), lane_masks)
            inner_ref[here] = dot(lower_ref[here] * level, rounded).astype(BF16)
        for here in chunks:
            inverse = inverse_ref[here]
            inner = block_diagonal(inner_ref[here], lane_masks)
            inverse_ref[here] = inverse - dot(inverse.astype(BF16), inner)
        size = 2 * BASE
        while size < HEAD:
            odd = range(size, HEAD, 2 * size)
            block = iota((size, width), 1) % HEAD // size
            gap = jnp.zeros((size, width), BF16)
            for n in range(count):
                rounded = block_diagonal(inverse_ref[chunks[n]].astype(BF16), lane_masks)
                off = [
                    jnp.where(block == r // size - 1, lower_ref[pl.ds(n * HEAD + r, size)], gap) for r in odd
                ]
                inner_ref[pl.ds(n * HEAD, HEAD // 2)] = dot(jnp.concatenate(off, axis=0), rounded).astype(BF16)
            for n in range(count):
                inner = []
                for i, r in enumerate(odd):
                    inner += [gap, inner_ref[pl.ds(n * HEAD + i * size, size)]]
                inner = block_diagonal(jnp.concatenate(inner, axis=0), lane_masks)
                places = [pl.ds(n * HEAD + r, size) for r in odd]
                inverse = jnp.concatenate([inverse_ref[p] for p in places], axis=0)
                inverse = inverse - dot(inverse.astype(BF16), inner)
                for i, p in enumerate(places):
                    inverse_ref[p] = inverse[i * size : (i + 1) * size]
            size *= 2
        for n, here in enumerate(chunks):
            inverse = block_diagonal(inverse_ref[here].astype(BF16), lane_masks)
            turned = (turned_ref[here].astype(F32) * chunk_row(beta, n, heads)).astype(BF16)
            inner_ref[here] = dot(turned, inverse).astype(BF16)
        for here in chunks:
            added = (silu(kv_acc[here, width:].astype(BF16).astype(F32)) * wide_ref[here]).astype(BF16)
            for f in range(0, width, 128):
                both = jnp.concatenate([key_ref[here, f : f + 128], added[:, f : f + 128]], axis=1)
                map_ref[here, 2 * f : 2 * f + 256] = dot(inner_ref[here, f : f + 128], pair_diagonal(both, lane_masks))
        reach = 1
        while reach < span:
            for n in range(0, count, 2 * reach):
                early, late = chunks[n], chunks[n + reach]
                for f in range(0, 2 * width, 256):
                    before, later = map_ref[early, f : f + 256], map_ref[late, f : f + 256]
                    carried = dot(later[:, :128].astype(BF16), pair_diagonal(before.astype(BF16), lane_masks))
                    map_ref[early, f : f + 256] = before + later - carried
            reach *= 2

        lane_head = iota((1, width), 1) // HEAD
        maps = []
        for s in range(seqs):
            here = chunks[s * span]
            keep = jnp.zeros((1, width), F32)
            for h in range(heads):
                keep = jnp.where(lane_head == h, kept[s][h : h + 1], keep)
            tiles = []
            for f in range(0, width, 128):
                part = slice(f, f + 128)
                removal = keep[:, part] * map_ref[here, 2 * f : 2 * f + 128]
                tiles.append(removal + jnp.where(row[:, part] == column[:, part], 1.0 - keep[:, part], 0.0))
                tiles.append(map_ref[here, 2 * f + 128 : 2 * f + 256])
            maps.append(jnp.concatenate(tiles, axis=1))
        shared_out(place_ref[1] % 2, maps, kept_ref, sent_ref)


def shared_out(bit, halves, kept_ref, sent_ref):
    kept_ref[...] = jnp.where(bit == 0, halves[0], halves[1])
    sent_ref[...] = jnp.where(bit == 0, halves[1], halves[0])


def in_order(bit, own, other):
    return jnp.where(bit == 0, other, own), jnp.where(bit == 0, own, other)


def pair_after(later, earlier):
    lane_masks = head_masks()
    high, low = split(later[:, :128])
    first_high, first_low = split(earlier)
    product = dot(jnp.concatenate([high, low], axis=1), jnp.concatenate([pair_diagonal(first_high, lane_masks)] * 2, axis=0))
    return earlier + later - (product + dot(high, pair_diagonal(first_low, lane_masks)))


def widened(x):
    x = jnp.where(iota(x.shape, 1) < HEAD, x, 0.0)
    high = x.astype(BF16)
    low = lanes_turned(x - high.astype(F32), HEAD).astype(BF16)
    return jnp.concatenate([high + low, high], axis=1)


def stacked(x):
    high, low = split(x)
    return jnp.concatenate([high, high, low, low], axis=0)


def first_kernel(place_ref, own_ref, other_ref, kept_ref, sent_ref):
    later, earlier = in_order(place_ref[0] % 2, own_ref[...], other_ref[...])
    pairs = [pair_after(later[:, f : f + 256], earlier[:, f : f + 256]) for f in range(0, later.shape[1], 256)]
    shared_out(place_ref[0] // 2 % 2, pairs, kept_ref, sent_ref)


def second_kernel(place_ref, own_ref, other_ref, kept_ref, sent_ref):
    pair = pair_after(*in_order(place_ref[0] // 2 % 2, own_ref[...], other_ref[...]))
    removal, offset = pair[:, :128], pair[:, 128:]
    low_lanes = iota(removal.shape, 1) < HEAD
    even = jnp.where(low_lanes, removal, lanes_turned(offset, HEAD))
    odd = jnp.where(low_lanes, lanes_turned(removal, HEAD), offset)
    shared_out(place_ref[0] // 4 % 2, (even, odd), kept_ref, sent_ref)


def third_kernel(heads, place_ref, probe_ref, own_ref, other_ref, out_ref):
    place = place_ref[0]
    later, earlier = in_order(place // 4 % 2, own_ref[...], other_ref[...])
    state = earlier + later - dot(widened(later), stacked(earlier))
    shape = state.shape
    through = jnp.where(iota(shape, 0) == iota(shape, 1), 1.0 - state, -state)
    through = jnp.where(iota(shape, 1) < HEAD, through, state)
    probe = probe_ref[...].astype(F32)
    probe = jnp.sum(jnp.where(iota(probe.shape, 0) == place % 2, probe, 0.0), axis=0, keepdims=True)
    head = place // 2 % 2 * 2 + place // 4 % 2
    query = jnp.zeros((1, 128), F32)
    for h in range(heads):
        pair = probe[:, 128 * (h // 2) : 128 * (h // 2 + 1)]
        query = jnp.where(head == h, lanes_turned(pair, HEAD) if h % 2 else pair, query)
    query = jnp.broadcast_to(query[:, :HEAD], (8, HEAD)).astype(BF16)
    read = jnp.zeros((8, 128), F32)
    rest = through
    for _ in range(3):
        piece = rest.astype(BF16)
        read = read + dot(query, piece)
        rest = rest - piece.astype(F32)
    half = HEAD // 2
    packed = jnp.where(iota((half, 128), 1) < HEAD, lanes_turned(state[:half], HEAD), state[half:])
    ways = out_ref.shape[0]
    share = HEAD // ways
    is_late = place >= ways // 2
    for j in range(ways):
        rows = jnp.concatenate([through[share * j : share * (j + 1)], read[share:]], axis=0)
        out_ref[j, :8] = jnp.where(is_late, rows, packed[:8])
        out_ref[j, 8:] = packed[8:]


def result_kernel(in_ref, rows_ref, read_ref):
    seqs, heads, share, _ = rows_ref.shape
    ways = in_ref.shape[0]
    lane = iota((8, 128), 1)
    reads = []
    for g in range(seqs * heads):
        source = g // heads + g % heads // 2 * 2 + g % 2 * 4
        late = in_ref[source + ways // 2, :8]
        packed = in_ref[source]
        early = jnp.concatenate([packed, lanes_turned(packed, HEAD)], axis=0)
        both = dot(widened(late), stacked(early)) + lanes_turned(late, HEAD)
        rows_ref[g // heads, g % heads] = both[:share, :HEAD].astype(BF16)
        read = jnp.where(lane < HEAD, both, 0.0)[share : share + 1]
        mean = jnp.sum(read * read, axis=1, keepdims=True) / HEAD
        reads.append(read * lax.rsqrt(mean + 1e-06))
    for s in range(seqs):
        own = reads[s * heads : (s + 1) * heads]
        pairs = [own[h] + lanes_turned(own[h + 1], HEAD) for h in range(0, heads, 2)]
        read_ref[pl.ds(s, 1)] = jnp.concatenate(pairs, axis=1).astype(BF16)


def head_masks():
    low_lanes = iota((HEAD, 128), 1) < HEAD
    return [jnp.where(low_lanes, 1.0, 0.0).astype(BF16), jnp.where(low_lanes, 0.0, 1.0).astype(BF16)]


def body(
    layer_feed,
    address_mapping,
    content_mapping,
    beta_mapping_matrix,
    forgetting_mapping,
    logged_fading_speed,
    extra_forgetting,
    opening_probe,
):
    seqs, length, depth = layer_feed.shape
    width = address_mapping.shape[1]
    heads = width // HEAD
    all_heads = beta_mapping_matrix.shape[1]
    tokens = seqs * length
    ways = lax.axis_size("sp")
    steps = 4
    deep = depth // steps
    turn = lax.axis_index("sp").astype(jnp.int32).reshape(1)
    place = jnp.concatenate([lax.axis_index("tp").astype(jnp.int32).reshape(1), turn])
    share = (HEAD, 2 * width)
    kept, sent = pl.pallas_call(
        functools.partial(local_kernel, heads),
        grid=(steps,),
        out_shape=(jax.ShapeDtypeStruct(share, F32),) * 2,
        in_specs=[
            pl.BlockSpec(memory_space=pltpu.SMEM),
            pl.BlockSpec(memory_space=pltpu.SMEM),
            pl.BlockSpec((seqs, length, deep), lambda i: (0, 0, i)),
            pl.BlockSpec((deep, width), lambda i: (i, 0)),
            pl.BlockSpec((deep, width), lambda i: (i, 0)),
            pl.BlockSpec((all_heads, deep), lambda i: (0, i)),
            pl.BlockSpec((all_heads, deep), lambda i: (0, i)),
            pl.BlockSpec((seqs, heads, length), lambda i: (0, 0, 0)),
        ],
        out_specs=(pl.BlockSpec(share, lambda i: (0, 0)),) * 2,
        scratch_shapes=[
            pltpu.VMEM((tokens, 2 * width), F32),
            pltpu.VMEM((2 * all_heads, tokens), F32),
            pltpu.VMEM((tokens, width), F32),
            pltpu.VMEM((tokens, width), BF16),
            pltpu.VMEM((tokens, width), BF16),
            pltpu.VMEM((tokens, width), BF16),
            pltpu.VMEM((tokens, width), F32),
            pltpu.VMEM((tokens, width), BF16),
            pltpu.VMEM((tokens, 2 * width), F32),
            pltpu.VMEM((tokens * width // HEAD // 128 * BASE, 128), F32),
            pltpu.VMEM((tokens * width // HEAD // 128 * BASE, 128 * (BASE - 1)), F32),
        ],
        compiler_params=pltpu.CompilerParams(vmem_limit_bytes=63 << 20),
        name="local_maps",
    )(
        place,
        logged_fading_speed,
        layer_feed,
        address_mapping,
        content_mapping,
        beta_mapping_matrix.T,
        forgetting_mapping.T,
        extra_forgetting.transpose(0, 2, 1),
    )
    scalar, vector = pl.BlockSpec(memory_space=pltpu.SMEM), pl.BlockSpec(memory_space=pltpu.VMEM)
    small = pltpu.CompilerParams(vmem_limit_bytes=8 << 20)

    def swapped(x, distance):
        return lax.ppermute(x, "sp", [(i, i ^ distance) for i in range(ways)])

    for kernel, distance, lanes, name in ((first_kernel, 1, width, "first"), (second_kernel, 2, width // 2, "second")):
        kept, sent = pl.pallas_call(
            kernel,
            out_shape=(jax.ShapeDtypeStruct((HEAD, lanes), F32),) * 2,
            in_specs=[scalar, vector, vector],
            compiler_params=small,
            name=name,
        )(turn, kept, swapped(sent, distance))
    shares = pl.pallas_call(
        functools.partial(third_kernel, heads),
        out_shape=jax.ShapeDtypeStruct((ways, HEAD // 2, 128), F32),
        in_specs=[scalar, vector, vector, vector],
        compiler_params=small,
        name="third",
    )(turn, opening_probe, kept, swapped(sent, 4))
    mine = lax.all_to_all(shares, "sp", 0, 0, tiled=True)
    return pl.pallas_call(
        result_kernel,
        out_shape=(
            jax.ShapeDtypeStruct((seqs, heads, HEAD // ways, HEAD), BF16),
            jax.ShapeDtypeStruct((seqs, width), BF16),
        ),
        compiler_params=pltpu.CompilerParams(vmem_limit_bytes=8 << 20),
        name="results",
    )(mine)


def solution(mesh):
    in_specs = (
        P("grp", "sp", None),
        P(None, "tp"),
        P(None, "tp"),
        P(),
        P(),
        P("tp"),
        P("grp", "sp", "tp"),
        P("grp", "tp"),
    )
    out_specs = (P("grp", "tp", "sp", None), P("grp", "tp"))
    return jax.shard_map(body, mesh=mesh, in_specs=in_specs, out_specs=out_specs, check_vma=False)
```

```python
import functools

import jax
import jax.numpy as jnp
from jax import lax
from jax.experimental import pallas as pl
from jax.experimental.pallas import tpu as pltpu
from jax.sharding import PartitionSpec as P

HEAD = 64
BASE = 8
F32 = jnp.float32
BF16 = jnp.bfloat16


def iota(shape, dim):
    return lax.broadcasted_iota(jnp.int32, shape, dim)


def silu(v):
    return v / (1.0 + jnp.exp(-v))


def dot(a, b, dims=(1, 0)):
    return lax.dot_general(a, b, (((dims[0],), (dims[1],)), ((), ())), preferred_element_type=F32)


def lanes_turned(x, amount):
    amount %= x.shape[1]
    return pltpu.roll(x, amount, 1) if amount else x


def split(x):
    high = x.astype(BF16)
    return high, (x - high.astype(F32)).astype(BF16)


def block_diagonal(x, lane_masks):
    heads = x.shape[1] // HEAD
    empty = jnp.zeros((x.shape[0], 128), x.dtype)
    rows = []
    for h in range(heads):
        pair = h // 2
        own = x[:, 128 * pair : 128 * (pair + 1)] * lane_masks[h % 2]
        rows.append(jnp.concatenate([own if p == pair else empty for p in range(heads // 2)], axis=1))
    return jnp.concatenate(rows, axis=0)


def pair_diagonal(x, lane_masks):
    tiles = [x[:, f : f + 128] for f in range(0, x.shape[1], 128)]
    return jnp.concatenate(
        [jnp.concatenate([t * lane_masks[h] for t in tiles], axis=1) for h in range(2)], axis=0
    )


def chunk_row(x, n, heads):
    here = x[:, 128 * (n // 2) : 128 * (n // 2 + 1)]
    turned = lanes_turned(here, HEAD)
    left, right = (here, turned) if n % 2 == 0 else (turned, here)
    first = iota((1, 128), 1) < HEAD
    return jnp.concatenate(
        [jnp.where(first, left[h : h + 1], right[h + 1 : h + 2]) for h in range(0, heads, 2)], axis=1
    )


def diagonal_blocks(x):
    block = iota((BASE, x.shape[1]), 1) % HEAD // BASE
    blocks = x[:BASE]
    for r in range(1, HEAD // BASE):
        blocks = jnp.where(block == r, x[BASE * r : BASE * (r + 1)], blocks)
    return blocks


def composed(parts, combine):
    while len(parts) > 1:
        joined = [combine(parts[i + 1], parts[i]) for i in range(0, len(parts) - 1, 2)]
        parts = joined + parts[len(joined) * 2 :]
    return parts[0]


def local_kernel(
    heads, place_ref, turn_ref, speed_ref, x_ref, wk_ref, wv_ref, wb_ref, wf_ref, extra_ref, kept_ref, sent_ref,
    kv_acc, small_acc, wide_ref, turned_ref, key_ref, lower_ref, inverse_ref, inner_ref, map_ref,
    blocks_ref, factor_ref
):
    step = pl.program_id(0)
    width = heads * HEAD
    seqs, length, deep = x_ref.shape
    tokens = seqs * length
    all_heads = wb_ref.shape[0]

    @pl.when(step == 0)
    def _():
        kv_acc[...] = jnp.zeros_like(kv_acc)
        small_acc[...] = jnp.zeros_like(small_acc)

    x = x_ref[...].reshape(tokens, deep)
    kv_acc[:, :width] += dot(x, wk_ref[...])
    kv_acc[:, width:] += dot(x, wv_ref[...])
    small_acc[...] += dot(jnp.concatenate([wb_ref[...], wf_ref[...]], axis=0), x, (1, 1))

    @pl.when(step == pl.num_programs(0) - 1)
    def _():
        first = place_ref[0] * heads
        half = 2 * heads
        head_of_row = iota((half, 2 * all_heads), 0) % heads
        column = iota((half, 2 * all_heads), 1)
        small = small_acc[...].astype(BF16)
        beta_pre = dot(jnp.where(column == first + head_of_row, 1.0, 0.0).astype(BF16), small)
        decay_pre = dot(jnp.where(column == all_heads + first + head_of_row, 1.0, 0.0).astype(BF16), small)
        twice = jnp.where(iota((half, heads), 0) % heads == iota((half, heads), 1), 1.0, 0.0).astype(BF16)
        row_head = iota((half, 1), 0) % heads
        speed = jnp.zeros((half, 1), F32)
        for h in range(heads):
            speed = jnp.where(row_head == h, speed_ref[h], speed)
        rate = jnp.exp(speed)
        soft = jnp.maximum(decay_pre, 0.0) + jnp.log1p(jnp.exp(-jnp.abs(decay_pre)))
        beta = 1.0 / (1.0 + jnp.exp(-beta_pre))
        gammas = [
            dot(twice, extra_ref[s]) - rate * soft[:, s * length : (s + 1) * length] for s in range(seqs)
        ]
        behind_it = jnp.where(iota((length, length), 0) > iota((length, length), 1), 1.0, 0.0).astype(BF16)
        pieces = []
        for gamma in gammas:
            for _ in range(3):
                pieces.append(gamma.astype(BF16).astype(F32))
                gamma = gamma - pieces[-1]
        sums = dot(jnp.concatenate(pieces, axis=0).astype(BF16), behind_it)
        decays, kept = [], []
        for s in range(seqs):
            own = sums[3 * half * s : 3 * half * (s + 1)]
            behind = own[:half] + own[half : 2 * half] + own[2 * half :]
            decays.append(jnp.exp(behind))
            kept.append(jnp.exp(gammas[s][:, :1] + behind[:, :1]))
        stack = jnp.concatenate([p.astype(F32) for p in split(jnp.concatenate(decays, axis=1))], axis=0)
        pick = iota((2 * half, width), 0) % half == iota((2 * half, width), 1) // HEAD
        wide_ref[...] = dot(stack.T.astype(BF16), jnp.where(pick, 1.0, 0.0).astype(BF16))

        low_lanes = iota((HEAD, 128), 1) < HEAD
        lane_masks = [jnp.where(low_lanes, 1.0, 0.0).astype(BF16), jnp.where(low_lanes, 0.0, 1.0).astype(BF16)]
        same_head = iota((width, width), 0) // HEAD == iota((width, width), 1) // HEAD
        ones = jnp.where(same_head, 1.0, 0.0).astype(BF16)
        count = tokens // HEAD
        span = length // HEAD
        chunks = [pl.ds(n * HEAD, HEAD) for n in range(count)]
        for n in range(0, count, 2):
            here = pl.ds(n * HEAD, 2 * HEAD)
            keys = silu(kv_acc[here, :width].astype(BF16).astype(F32))
            norm = dot((keys * keys).astype(BF16), ones)
            keys = keys * lax.rsqrt(norm + 1e-06)
            key_ref[here] = keys.astype(BF16)
            turned = keys.astype(BF16).T
            for c in range(2):
                turned_ref[chunks[n + c]] = jnp.concatenate(
                    [turned[HEAD * h : HEAD * (h + 1), HEAD * c : HEAD * (c + 1)] for h in range(heads)], axis=1
                )
        row, column = iota((HEAD, width), 0), iota((HEAD, width), 1) % HEAD
        for n, here in enumerate(chunks):
            lower = dot(key_ref[here], block_diagonal(turned_ref[here], lane_masks))
            lower = jnp.where(row > column, lower * chunk_row(beta, n, heads), 0.0)
            lower_ref[here] = lower.astype(BF16)
            blocks = diagonal_blocks(lower)
            for f in range(0, width, 128):
                blocks_ref[pl.ds((n * width + f) // 128 * BASE, BASE)] = blocks[:, f : f + 128]
        spread_row, spread_col = iota((128, 128), 0), iota((128, 128), 1)
        spread = jnp.concatenate(
            [
                jnp.where(spread_row == spread_col // BASE * BASE + m, 1.0, 0.0).astype(BF16)
                for m in range(BASE - 1)
            ],
            axis=1,
        )
        factor_ref[...] = dot(blocks_ref[...].astype(BF16), spread)
        sets = blocks_ref.shape[0] // BASE
        solved = jnp.where(iota((BASE, 128), 0) == iota((BASE, 128), 1) % BASE, 1.0, 0.0)
        solved = jnp.broadcast_to(solved[None], (sets, BASE, 128))
        for m in range(BASE - 1):
            factor = factor_ref[:, 128 * m : 128 * (m + 1)].reshape(sets, BASE, 128)
            solved = solved - factor * solved[:, m : m + 1]
        blocks_ref[...] = solved.reshape(sets * BASE, 128)
        block = iota((BASE, width), 1) % HEAD // BASE
        for n, here in enumerate(chunks):
            own = jnp.concatenate(
                [blocks_ref[pl.ds((n * width + f) // 128 * BASE, BASE)] for f in range(0, width, 128)], axis=1
            )
            inverse_ref[here] = jnp.concatenate(
                [jnp.where(block == r, own, 0.0) for r in range(HEAD // BASE)], axis=0
            )
        level = (row // (2 * BASE) == column // (2 * BASE)) & (row // BASE > column // BASE)
        level = jnp.where(level, 1.0, 0.0).astype(BF16)
        for here in chunks:
            rounded = block_diagonal(inverse_ref[here].astype(BF16), lane_masks)
            inner_ref[here] = dot(lower_ref[here] * level, rounded).astype(BF16)
        for here in chunks:
            inverse = inverse_ref[here]
            inner = block_diagonal(inner_ref[here], lane_masks)
            inverse_ref[here] = inverse - dot(inverse.astype(BF16), inner)
        size = 2 * BASE
        while size < HEAD:
            odd = range(size, HEAD, 2 * size)
            block = iota((size, width), 1) % HEAD // size
            gap = jnp.zeros((size, width), BF16)
            for n in range(count):
                rounded = block_diagonal(inverse_ref[chunks[n]].astype(BF16), lane_masks)
                off = [
                    jnp.where(block == r // size - 1, lower_ref[pl.ds(n * HEAD + r, size)], gap) for r in odd
                ]
                inner_ref[pl.ds(n * HEAD, HEAD // 2)] = dot(jnp.concatenate(off, axis=0), rounded).astype(BF16)
            for n in range(count):
                inner = []
                for i, r in enumerate(odd):
                    inner += [gap, inner_ref[pl.ds(n * HEAD + i * size, size)]]
                inner = block_diagonal(jnp.concatenate(inner, axis=0), lane_masks)
                places = [pl.ds(n * HEAD + r, size) for r in odd]
                inverse = jnp.concatenate([inverse_ref[p] for p in places], axis=0)
                inverse = inverse - dot(inverse.astype(BF16), inner)
                for i, p in enumerate(places):
                    inverse_ref[p] = inverse[i * size : (i + 1) * size]
            size *= 2
        for n, here in enumerate(chunks):
            inverse = block_diagonal(inverse_ref[here].astype(BF16), lane_masks)
            turned = (turned_ref[here].astype(F32) * chunk_row(beta, n, heads)).astype(BF16)
            inner_ref[here] = dot(turned, inverse).astype(BF16)
        for here in chunks:
            added = (silu(kv_acc[here, width:].astype(BF16).astype(F32)) * wide_ref[here]).astype(BF16)
            for f in range(0, width, 128):
                both = jnp.concatenate([key_ref[here, f : f + 128], added[:, f : f + 128]], axis=1)
                map_ref[here, 2 * f : 2 * f + 256] = dot(inner_ref[here, f : f + 128], pair_diagonal(both, lane_masks))
        reach = 1
        while reach < span:
            for n in range(0, count, 2 * reach):
                early, late = chunks[n], chunks[n + reach]
                for f in range(0, 2 * width, 256):
                    before, later = map_ref[early, f : f + 256], map_ref[late, f : f + 256]
                    carried = dot(later[:, :128].astype(BF16), pair_diagonal(before.astype(BF16), lane_masks))
                    map_ref[early, f : f + 256] = before + later - carried
            reach *= 2

        lane_head = iota((1, width), 1) // HEAD
        maps = []
        for s in range(seqs):
            here = chunks[s * span]
            keep = jnp.zeros((1, width), F32)
            for h in range(heads):
                keep = jnp.where(lane_head == h, kept[s][h : h + 1], keep)
            tiles = []
            for f in range(0, width, 128):
                part = slice(f, f + 128)
                removal = keep[:, part] * map_ref[here, 2 * f : 2 * f + 128]
                tiles.append(removal + jnp.where(row[:, part] == column[:, part], 1.0 - keep[:, part], 0.0))
                tiles.append(map_ref[here, 2 * f + 128 : 2 * f + 256])
            maps.append(jnp.concatenate(tiles, axis=1))
        shared_out(turn_ref[0] % 2, maps, kept_ref, sent_ref)


def shared_out(bit, halves, kept_ref, sent_ref):
    kept_ref[...] = jnp.where(bit == 0, halves[0], halves[1])
    sent_ref[...] = jnp.where(bit == 0, halves[1], halves[0])


def in_order(bit, own, other):
    return jnp.where(bit == 0, other, own), jnp.where(bit == 0, own, other)


def pair_after(later, earlier):
    lane_masks = head_masks()
    high, low = split(later[:, :128])
    first_high, first_low = split(earlier)
    product = dot(jnp.concatenate([high, low], axis=1), jnp.concatenate([pair_diagonal(first_high, lane_masks)] * 2, axis=0))
    return earlier + later - (product + dot(high, pair_diagonal(first_low, lane_masks)))


def widened(x):
    x = jnp.where(iota(x.shape, 1) < HEAD, x, 0.0)
    high = x.astype(BF16)
    low = lanes_turned(x - high.astype(F32), HEAD).astype(BF16)
    return jnp.concatenate([high + low, high], axis=1)


def stacked(x):
    high, low = split(x)
    return jnp.concatenate([high, high, low, low], axis=0)


def first_kernel(place_ref, own_ref, other_ref, kept_ref, sent_ref):
    later, earlier = in_order(place_ref[0] % 2, own_ref[...], other_ref[...])
    pairs = [pair_after(later[:, f : f + 256], earlier[:, f : f + 256]) for f in range(0, later.shape[1], 256)]
    shared_out(place_ref[0] // 2 % 2, pairs, kept_ref, sent_ref)


def second_kernel(place_ref, own_ref, other_ref, kept_ref, sent_ref):
    pair = pair_after(*in_order(place_ref[0] // 2 % 2, own_ref[...], other_ref[...]))
    removal, offset = pair[:, :128], pair[:, 128:]
    low_lanes = iota(removal.shape, 1) < HEAD
    even = jnp.where(low_lanes, removal, lanes_turned(offset, HEAD))
    odd = jnp.where(low_lanes, lanes_turned(removal, HEAD), offset)
    shared_out(place_ref[0] // 4 % 2, (even, odd), kept_ref, sent_ref)


def third_kernel(heads, place_ref, probe_ref, own_ref, other_ref, out_ref):
    place = place_ref[0]
    later, earlier = in_order(place // 4 % 2, own_ref[...], other_ref[...])
    state = earlier + later - dot(widened(later), stacked(earlier))
    shape = state.shape
    through = jnp.where(iota(shape, 0) == iota(shape, 1), 1.0 - state, -state)
    through = jnp.where(iota(shape, 1) < HEAD, through, state)
    probe = probe_ref[...].astype(F32)
    probe = jnp.sum(jnp.where(iota(probe.shape, 0) == place % 2, probe, 0.0), axis=0, keepdims=True)
    head = place // 2 % 2 * 2 + place // 4 % 2
    query = jnp.zeros((1, 128), F32)
    for h in range(heads):
        pair = probe[:, 128 * (h // 2) : 128 * (h // 2 + 1)]
        query = jnp.where(head == h, lanes_turned(pair, HEAD) if h % 2 else pair, query)
    query = jnp.broadcast_to(query[:, :HEAD], (8, HEAD)).astype(BF16)
    read = jnp.zeros((8, 128), F32)
    rest = through
    for _ in range(3):
        piece = rest.astype(BF16)
        read = read + dot(query, piece)
        rest = rest - piece.astype(F32)
    half = HEAD // 2
    packed = jnp.where(iota((half, 128), 1) < HEAD, lanes_turned(state[:half], HEAD), state[half:])
    ways = out_ref.shape[0]
    share = HEAD // ways
    is_late = place >= ways // 2
    for j in range(ways):
        rows = jnp.concatenate([through[share * j : share * (j + 1)], read[share:]], axis=0)
        out_ref[j, :8] = jnp.where(is_late, rows, packed[:8])
        out_ref[j, 8:] = packed[8:]


def result_kernel(in_ref, rows_ref, read_ref):
    seqs, heads, share, _ = rows_ref.shape
    ways = in_ref.shape[0]
    lane = iota((8, 128), 1)
    reads = []
    for g in range(seqs * heads):
        source = g // heads + g % heads // 2 * 2 + g % 2 * 4
        late = in_ref[source + ways // 2, :8]
        packed = in_ref[source]
        early = jnp.concatenate([packed, lanes_turned(packed, HEAD)], axis=0)
        both = dot(widened(late), stacked(early)) + lanes_turned(late, HEAD)
        rows_ref[g // heads, g % heads] = both[:share, :HEAD].astype(BF16)
        read = jnp.where(lane < HEAD, both, 0.0)[share : share + 1]
        mean = jnp.sum(read * read, axis=1, keepdims=True) / HEAD
        reads.append(read * lax.rsqrt(mean + 1e-06))
    for s in range(seqs):
        own = reads[s * heads : (s + 1) * heads]
        pairs = [own[h] + lanes_turned(own[h + 1], HEAD) for h in range(0, heads, 2)]
        read_ref[pl.ds(s, 1)] = jnp.concatenate(pairs, axis=1).astype(BF16)


def head_masks():
    low_lanes = iota((HEAD, 128), 1) < HEAD
    return [jnp.where(low_lanes, 1.0, 0.0).astype(BF16), jnp.where(low_lanes, 0.0, 1.0).astype(BF16)]


def body(
    layer_feed,
    address_mapping,
    content_mapping,
    beta_mapping_matrix,
    forgetting_mapping,
    logged_fading_speed,
    extra_forgetting,
    opening_probe,
):
    seqs, length, depth = layer_feed.shape
    width = address_mapping.shape[1]
    heads = width // HEAD
    all_heads = beta_mapping_matrix.shape[1]
    tokens = seqs * length
    ways = lax.axis_size("sp")
    steps = 4
    deep = depth // steps
    turn = lax.axis_index("sp").astype(jnp.int32).reshape(1)
    place = lax.axis_index("tp").astype(jnp.int32).reshape(1)
    share = (HEAD, 2 * width)
    kept, sent = pl.pallas_call(
        functools.partial(local_kernel, heads),
        grid=(steps,),
        out_shape=(jax.ShapeDtypeStruct(share, F32),) * 2,
        in_specs=[
            pl.BlockSpec(memory_space=pltpu.SMEM),
            pl.BlockSpec(memory_space=pltpu.SMEM),
            pl.BlockSpec(memory_space=pltpu.SMEM),
            pl.BlockSpec((seqs, length, deep), lambda i: (0, 0, i)),
            pl.BlockSpec((deep, width), lambda i: (i, 0)),
            pl.BlockSpec((deep, width), lambda i: (i, 0)),
            pl.BlockSpec((all_heads, deep), lambda i: (0, i)),
            pl.BlockSpec((all_heads, deep), lambda i: (0, i)),
            pl.BlockSpec((seqs, heads, length), lambda i: (0, 0, 0)),
        ],
        out_specs=(pl.BlockSpec(share, lambda i: (0, 0)),) * 2,
        scratch_shapes=[
            pltpu.VMEM((tokens, 2 * width), F32),
            pltpu.VMEM((2 * all_heads, tokens), F32),
            pltpu.VMEM((tokens, width), F32),
            pltpu.VMEM((tokens, width), BF16),
            pltpu.VMEM((tokens, width), BF16),
            pltpu.VMEM((tokens, width), BF16),
            pltpu.VMEM((tokens, width), F32),
            pltpu.VMEM((tokens, width), BF16),
            pltpu.VMEM((tokens, 2 * width), F32),
            pltpu.VMEM((tokens * width // HEAD // 128 * BASE, 128), F32),
            pltpu.VMEM((tokens * width // HEAD // 128 * BASE, 128 * (BASE - 1)), F32),
        ],
        compiler_params=pltpu.CompilerParams(vmem_limit_bytes=63 << 20),
        name="local_maps",
    )(
        place,
        turn,
        logged_fading_speed,
        layer_feed,
        address_mapping,
        content_mapping,
        beta_mapping_matrix.T,
        forgetting_mapping.T,
        extra_forgetting.transpose(0, 2, 1),
    )
    scalar, vector = pl.BlockSpec(memory_space=pltpu.SMEM), pl.BlockSpec(memory_space=pltpu.VMEM)
    small = pltpu.CompilerParams(vmem_limit_bytes=8 << 20)

    def swapped(x, distance):
        return lax.ppermute(x, "sp", [(i, i ^ distance) for i in range(ways)])

    for kernel, distance, lanes, name in ((first_kernel, 1, width, "first"), (second_kernel, 2, width // 2, "second")):
        kept, sent = pl.pallas_call(
            kernel,
            out_shape=(jax.ShapeDtypeStruct((HEAD, lanes), F32),) * 2,
            in_specs=[scalar, vector, vector],
            compiler_params=small,
            name=name,
        )(turn, kept, swapped(sent, distance))
    shares = pl.pallas_call(
        functools.partial(third_kernel, heads),
        out_shape=jax.ShapeDtypeStruct((ways, HEAD // 2, 128), F32),
        in_specs=[scalar, vector, vector, vector],
        compiler_params=small,
        name="third",
    )(turn, opening_probe, kept, swapped(sent, 4))
    mine = lax.all_to_all(shares, "sp", 0, 0, tiled=True)
    return pl.pallas_call(
        result_kernel,
        out_shape=(
            jax.ShapeDtypeStruct((seqs, heads, HEAD // ways, HEAD), BF16),
            jax.ShapeDtypeStruct((seqs, width), BF16),
        ),
        compiler_params=pltpu.CompilerParams(vmem_limit_bytes=8 << 20),
        name="results",
    )(mine)


def solution(mesh):
    in_specs = (
        P("grp", "sp", None),
        P(None, "tp"),
        P(None, "tp"),
        P(),
        P(),
        P("tp"),
        P("grp", "sp", "tp"),
        P("grp", "tp"),
    )
    out_specs = (P("grp", "tp", "sp", None), P("grp", "tp"))
    return jax.shard_map(body, mesh=mesh, in_specs=in_specs, out_specs=out_specs, check_vma=False)
```

```python
import functools

import jax
import jax.numpy as jnp
from jax import lax
from jax.experimental import pallas as pl
from jax.experimental.pallas import tpu as pltpu
from jax.sharding import PartitionSpec as P

HEAD = 64
BASE = 8
F32 = jnp.float32
BF16 = jnp.bfloat16


def iota(shape, dim):
    return lax.broadcasted_iota(jnp.int32, shape, dim)


def silu(v):
    return v / (1.0 + jnp.exp(-v))


def dot(a, b, dims=(1, 0)):
    return lax.dot_general(a, b, (((dims[0],), (dims[1],)), ((), ())), preferred_element_type=F32)


def lanes_turned(x, amount):
    amount %= x.shape[1]
    return pltpu.roll(x, amount, 1) if amount else x


def split(x):
    high = x.astype(BF16)
    return high, (x - high.astype(F32)).astype(BF16)


def block_diagonal(x, lane_masks):
    heads = x.shape[1] // HEAD
    empty = jnp.zeros((x.shape[0], 128), x.dtype)
    rows = []
    for h in range(heads):
        pair = h // 2
        own = x[:, 128 * pair : 128 * (pair + 1)] * lane_masks[h % 2]
        rows.append(jnp.concatenate([own if p == pair else empty for p in range(heads // 2)], axis=1))
    return jnp.concatenate(rows, axis=0)


def pair_diagonal(x, lane_masks):
    tiles = [x[:, f : f + 128] for f in range(0, x.shape[1], 128)]
    return jnp.concatenate(
        [jnp.concatenate([t * lane_masks[h] for t in tiles], axis=1) for h in range(2)], axis=0
    )


def chunk_row(x, n, heads):
    here = x[:, 128 * (n // 2) : 128 * (n // 2 + 1)]
    turned = lanes_turned(here, HEAD)
    left, right = (here, turned) if n % 2 == 0 else (turned, here)
    first = iota((1, 128), 1) < HEAD
    return jnp.concatenate(
        [jnp.where(first, left[h : h + 1], right[h + 1 : h + 2]) for h in range(0, heads, 2)], axis=1
    )


def diagonal_blocks(x):
    block = iota((BASE, x.shape[1]), 1) % HEAD // BASE
    blocks = x[:BASE]
    for r in range(1, HEAD // BASE):
        blocks = jnp.where(block == r, x[BASE * r : BASE * (r + 1)], blocks)
    return blocks


def composed(parts, combine):
    while len(parts) > 1:
        joined = [combine(parts[i + 1], parts[i]) for i in range(0, len(parts) - 1, 2)]
        parts = joined + parts[len(joined) * 2 :]
    return parts[0]


def local_kernel(
    heads, place_ref, turn_ref, speed_ref, x_ref, wk_ref, wv_ref, wb_ref, wf_ref, extra_ref, kept_ref, sent_ref,
    kv_acc, small_acc, wide_ref, turned_ref, key_ref, lower_ref, inverse_ref, inner_ref, map_ref,
    blocks_ref, factor_ref
):
    step = pl.program_id(0)
    width = heads * HEAD
    seqs, length, deep = x_ref.shape
    tokens = seqs * length
    all_heads = wb_ref.shape[0]

    @pl.when(step == 0)
    def _():
        kv_acc[...] = jnp.zeros_like(kv_acc)
        small_acc[...] = jnp.zeros_like(small_acc)

    x = x_ref[...].reshape(tokens, deep)
    kv_acc[:, :width] += dot(x, wk_ref[...])
    kv_acc[:, width:] += dot(x, wv_ref[...])
    small_acc[...] += dot(jnp.concatenate([wb_ref[...], wf_ref[...]], axis=0), x, (1, 1))

    @pl.when(step == pl.num_programs(0) - 1)
    def _():
        first = place_ref[0] * heads
        half = 2 * heads
        head_of_row = iota((half, 2 * all_heads), 0) % heads
        column = iota((half, 2 * all_heads), 1)
        small = small_acc[...].astype(BF16)
        beta_pre = dot(jnp.where(column == first + head_of_row, 1.0, 0.0).astype(BF16), small)
        decay_pre = dot(jnp.where(column == all_heads + first + head_of_row, 1.0, 0.0).astype(BF16), small)
        twice = jnp.where(iota((half, heads), 0) % heads == iota((half, heads), 1), 1.0, 0.0).astype(BF16)
        row_head = iota((half, 1), 0) % heads
        speed = jnp.zeros((half, 1), F32)
        for h in range(heads):
            speed = jnp.where(row_head == h, speed_ref[h], speed)
        rate = jnp.exp(speed)
        soft = jnp.maximum(decay_pre, 0.0) + jnp.log1p(jnp.exp(-jnp.abs(decay_pre)))
        beta = 1.0 / (1.0 + jnp.exp(-beta_pre))
        gammas = [
            dot(twice, extra_ref[s]) - rate * soft[:, s * length : (s + 1) * length] for s in range(seqs)
        ]
        behind_it = jnp.where(iota((length, length), 0) > iota((length, length), 1), 1.0, 0.0).astype(BF16)
        pieces = []
        for gamma in gammas:
            for _ in range(3):
                pieces.append(gamma.astype(BF16).astype(F32))
                gamma = gamma - pieces[-1]
        sums = dot(jnp.concatenate(pieces, axis=0).astype(BF16), behind_it)
        decays, kept = [], []
        for s in range(seqs):
            own = sums[3 * half * s : 3 * half * (s + 1)]
            behind = own[:half] + own[half : 2 * half] + own[2 * half :]
            decays.append(jnp.exp(behind))
            kept.append(jnp.exp(gammas[s][:, :1] + behind[:, :1]))
        stack = jnp.concatenate([p.astype(F32) for p in split(jnp.concatenate(decays, axis=1))], axis=0)
        pick = iota((2 * half, width), 0) % half == iota((2 * half, width), 1) // HEAD
        wide_ref[...] = dot(stack.T.astype(BF16), jnp.where(pick, 1.0, 0.0).astype(BF16))

        low_lanes = iota((HEAD, 128), 1) < HEAD
        lane_masks = [jnp.where(low_lanes, 1.0, 0.0).astype(BF16), jnp.where(low_lanes, 0.0, 1.0).astype(BF16)]
        same_head = iota((width, width), 0) // HEAD == iota((width, width), 1) // HEAD
        ones = jnp.where(same_head, 1.0, 0.0).astype(BF16)
        count = tokens // HEAD
        span = length // HEAD
        chunks = [pl.ds(n * HEAD, HEAD) for n in range(count)]
        for n in range(0, count, 2):
            here = pl.ds(n * HEAD, 2 * HEAD)
            keys = silu(kv_acc[here, :width].astype(BF16).astype(F32))
            norm = dot((keys * keys).astype(BF16), ones)
            keys = keys * lax.rsqrt(norm + 1e-06)
            key_ref[here] = keys.astype(BF16)
            turned = keys.astype(BF16).T
            for c in range(2):
                turned_ref[chunks[n + c]] = jnp.concatenate(
                    [turned[HEAD * h : HEAD * (h + 1), HEAD * c : HEAD * (c + 1)] for h in range(heads)], axis=1
                )
        row, column = iota((HEAD, width), 0), iota((HEAD, width), 1) % HEAD
        for n, here in enumerate(chunks):
            lower = dot(key_ref[here], block_diagonal(turned_ref[here], lane_masks))
            lower = jnp.where(row > column, lower * chunk_row(beta, n, heads), 0.0)
            lower_ref[here] = lower.astype(BF16)
            blocks = diagonal_blocks(lower)
            for f in range(0, width, 128):
                blocks_ref[pl.ds((n * width + f) // 128 * BASE, BASE)] = blocks[:, f : f + 128]
        spread_row, spread_col = iota((128, 128), 0), iota((128, 128), 1)
        spread = jnp.concatenate(
            [
                jnp.where(spread_row == spread_col // BASE * BASE + m, 1.0, 0.0).astype(BF16)
                for m in range(BASE - 1)
            ],
            axis=1,
        )
        factor_ref[...] = dot(blocks_ref[...].astype(BF16), spread)
        sets = blocks_ref.shape[0] // BASE
        solved = jnp.where(iota((BASE, 128), 0) == iota((BASE, 128), 1) % BASE, 1.0, 0.0)
        solved = jnp.broadcast_to(solved[None], (sets, BASE, 128))
        for m in range(BASE - 1):
            factor = factor_ref[:, 128 * m : 128 * (m + 1)].reshape(sets, BASE, 128)
            solved = solved - factor * solved[:, m : m + 1]
        blocks_ref[...] = solved.reshape(sets * BASE, 128)
        block = iota((BASE, width), 1) % HEAD // BASE
        for n, here in enumerate(chunks):
            own = jnp.concatenate(
                [blocks_ref[pl.ds((n * width + f) // 128 * BASE, BASE)] for f in range(0, width, 128)], axis=1
            )
            inverse_ref[here] = jnp.concatenate(
                [jnp.where(block == r, own, 0.0) for r in range(HEAD // BASE)], axis=0
            )
        level = (row // (2 * BASE) == column // (2 * BASE)) & (row // BASE > column // BASE)
        level = jnp.where(level, 1.0, 0.0).astype(BF16)
        for here in chunks:
            rounded = block_diagonal(inverse_ref[here].astype(BF16), lane_masks)
            inner_ref[here] = dot(lower_ref[here] * level, rounded).astype(BF16)
        for here in chunks:
            inverse = inverse_ref[here]
            inner = block_diagonal(inner_ref[here], lane_masks)
            inverse_ref[here] = inverse - dot(inverse.astype(BF16), inner)
        size = 2 * BASE
        while size < HEAD:
            odd = range(size, HEAD, 2 * size)
            block = iota((size, width), 1) % HEAD // size
            gap = jnp.zeros((size, width), BF16)
            for n in range(count):
                rounded = block_diagonal(inverse_ref[chunks[n]].astype(BF16), lane_masks)
                off = [
                    jnp.where(block == r // size - 1, lower_ref[pl.ds(n * HEAD + r, size)], gap) for r in odd
                ]
                inner_ref[pl.ds(n * HEAD, HEAD // 2)] = dot(jnp.concatenate(off, axis=0), rounded).astype(BF16)
            for n in range(count):
                inner = []
                for i, r in enumerate(odd):
                    inner += [gap, inner_ref[pl.ds(n * HEAD + i * size, size)]]
                inner = block_diagonal(jnp.concatenate(inner, axis=0), lane_masks)
                places = [pl.ds(n * HEAD + r, size) for r in odd]
                inverse = jnp.concatenate([inverse_ref[p] for p in places], axis=0)
                inverse = inverse - dot(inverse.astype(BF16), inner)
                for i, p in enumerate(places):
                    inverse_ref[p] = inverse[i * size : (i + 1) * size]
            size *= 2
        for n, here in enumerate(chunks):
            inverse = block_diagonal(inverse_ref[here].astype(BF16), lane_masks)
            turned = (turned_ref[here].astype(F32) * chunk_row(beta, n, heads)).astype(BF16)
            inner_ref[here] = dot(turned, inverse).astype(BF16)
        for here in chunks:
            added = (silu(kv_acc[here, width:].astype(BF16).astype(F32)) * wide_ref[here]).astype(BF16)
            for f in range(0, width, 128):
                both = jnp.concatenate([key_ref[here, f : f + 128], added[:, f : f + 128]], axis=1)
                map_ref[here, 2 * f : 2 * f + 256] = dot(inner_ref[here, f : f + 128], pair_diagonal(both, lane_masks))
        reach = 1
        while reach < span:
            for n in range(0, count, 2 * reach):
                early, late = chunks[n], chunks[n + reach]
                for f in range(0, 2 * width, 256):
                    before, later = map_ref[early, f : f + 256], map_ref[late, f : f + 256]
                    carried = dot(later[:, :128].astype(BF16), pair_diagonal(before.astype(BF16), lane_masks))
                    map_ref[early, f : f + 256] = before + later - carried
            reach *= 2

        lane_head = iota((1, width), 1) // HEAD
        maps = []
        for s in range(seqs):
            here = chunks[s * span]
            keep = jnp.zeros((1, width), F32)
            for h in range(heads):
                keep = jnp.where(lane_head == h, kept[s][h : h + 1], keep)
            tiles = []
            for f in range(0, width, 128):
                part = slice(f, f + 128)
                removal = keep[:, part] * map_ref[here, 2 * f : 2 * f + 128]
                tiles.append(removal + jnp.where(row[:, part] == column[:, part], 1.0 - keep[:, part], 0.0))
                tiles.append(map_ref[here, 2 * f + 128 : 2 * f + 256])
            maps.append(jnp.concatenate(tiles, axis=1))
        shared_out(turn_ref[0] % 2, maps, kept_ref, sent_ref)


def shared_out(bit, halves, kept_ref, sent_ref):
    kept_ref[...] = jnp.where(bit == 0, halves[0], halves[1])
    sent_ref[...] = jnp.where(bit == 0, halves[1], halves[0])


def in_order(bit, own, other):
    return jnp.where(bit == 0, other, own), jnp.where(bit == 0, own, other)


def pair_after(later, earlier):
    lane_masks = head_masks()
    high, low = split(later[:, :128])
    first_high, first_low = split(earlier)
    product = dot(jnp.concatenate([high, low], axis=1), jnp.concatenate([pair_diagonal(first_high, lane_masks)] * 2, axis=0))
    return earlier + later - (product + dot(high, pair_diagonal(first_low, lane_masks)))


def widened(x):
    x = jnp.where(iota(x.shape, 1) < HEAD, x, 0.0)
    high = x.astype(BF16)
    low = lanes_turned(x - high.astype(F32), HEAD).astype(BF16)
    return jnp.concatenate([high + low, high], axis=1)


def stacked(x):
    high, low = split(x)
    return jnp.concatenate([high, high, low, low], axis=0)


def first_kernel(place_ref, own_ref, other_ref, kept_ref, sent_ref):
    later, earlier = in_order(place_ref[0] % 2, own_ref[...], other_ref[...])
    pairs = [pair_after(later[:, f : f + 256], earlier[:, f : f + 256]) for f in range(0, later.shape[1], 256)]
    shared_out(place_ref[0] // 2 % 2, pairs, kept_ref, sent_ref)


def second_kernel(place_ref, own_ref, other_ref, kept_ref, sent_ref):
    pair = pair_after(*in_order(place_ref[0] // 2 % 2, own_ref[...], other_ref[...]))
    removal, offset = pair[:, :128], pair[:, 128:]
    low_lanes = iota(removal.shape, 1) < HEAD
    even = jnp.where(low_lanes, removal, lanes_turned(offset, HEAD))
    odd = jnp.where(low_lanes, lanes_turned(removal, HEAD), offset)
    shared_out(place_ref[0] // 4 % 2, (even, odd), kept_ref, sent_ref)


def third_kernel(heads, place_ref, probe_ref, own_ref, other_ref, out_ref):
    place = place_ref[0]
    later, earlier = in_order(place // 4 % 2, own_ref[...], other_ref[...])
    state = earlier + later - dot(widened(later), stacked(earlier))
    shape = state.shape
    through = jnp.where(iota(shape, 0) == iota(shape, 1), 1.0 - state, -state)
    through = jnp.where(iota(shape, 1) < HEAD, through, state)
    probe = probe_ref[...].astype(F32)
    probe = jnp.sum(jnp.where(iota(probe.shape, 0) == place % 2, probe, 0.0), axis=0, keepdims=True)
    head = place // 2 % 2 * 2 + place // 4 % 2
    query = jnp.zeros((1, 128), F32)
    for h in range(heads):
        pair = probe[:, 128 * (h // 2) : 128 * (h // 2 + 1)]
        query = jnp.where(head == h, lanes_turned(pair, HEAD) if h % 2 else pair, query)
    query = jnp.broadcast_to(query[:, :HEAD], (8, HEAD)).astype(BF16)
    read = jnp.zeros((8, 128), F32)
    rest = through
    for _ in range(3):
        piece = rest.astype(BF16)
        read = read + dot(query, piece)
        rest = rest - piece.astype(F32)
    half = HEAD // 2
    packed = jnp.where(iota((half, 128), 1) < HEAD, lanes_turned(state[:half], HEAD), state[half:])
    ways = out_ref.shape[0]
    share = HEAD // ways
    is_late = place >= ways // 2
    for j in range(ways):
        rows = jnp.concatenate([through[share * j : share * (j + 1)], read[share:]], axis=0)
        out_ref[j, :8] = jnp.where(is_late, rows, packed[:8])
        out_ref[j, 8:] = packed[8:]


def result_kernel(in_ref, rows_ref, read_ref):
    seqs, heads, share, _ = rows_ref.shape
    ways = in_ref.shape[0]
    lane = iota((8, 128), 1)
    reads = []
    for g in range(seqs * heads):
        source = g // heads + g % heads // 2 * 2 + g % 2 * 4
        late = in_ref[source + ways // 2, :8]
        packed = in_ref[source]
        early = jnp.concatenate([packed, lanes_turned(packed, HEAD)], axis=0)
        both = dot(widened(late), stacked(early)) + lanes_turned(late, HEAD)
        rows_ref[g // heads, g % heads] = both[:share, :HEAD].astype(BF16)
        read = jnp.where(lane < HEAD, both, 0.0)[share : share + 1]
        mean = jnp.sum(read * read, axis=1, keepdims=True) / HEAD
        reads.append(read * lax.rsqrt(mean + 1e-06))
    for s in range(seqs):
        own = reads[s * heads : (s + 1) * heads]
        pairs = [own[h] + lanes_turned(own[h + 1], HEAD) for h in range(0, heads, 2)]
        read_ref[pl.ds(s, 1)] = jnp.concatenate(pairs, axis=1).astype(BF16)


def head_masks():
    low_lanes = iota((HEAD, 128), 1) < HEAD
    return [jnp.where(low_lanes, 1.0, 0.0).astype(BF16), jnp.where(low_lanes, 0.0, 1.0).astype(BF16)]


def body(
    layer_feed,
    address_mapping,
    content_mapping,
    beta_mapping_matrix,
    forgetting_mapping,
    logged_fading_speed,
    extra_forgetting,
    opening_probe,
):
    seqs, length, depth = layer_feed.shape
    width = address_mapping.shape[1]
    heads = width // HEAD
    all_heads = beta_mapping_matrix.shape[1]
    tokens = seqs * length
    ways = lax.axis_size("sp")
    steps = 4
    deep = depth // steps
    turn = lax.axis_index("sp").astype(jnp.int32).reshape(1)
    place = lax.axis_index("tp").astype(jnp.int32).reshape(1)
    share = (HEAD, 2 * width)
    kept, sent = pl.pallas_call(
        functools.partial(local_kernel, heads),
        grid=(steps,),
        out_shape=(pltpu.VMEM(share, F32),) * 2,
        in_specs=[
            pl.BlockSpec(memory_space=pltpu.SMEM),
            pl.BlockSpec(memory_space=pltpu.SMEM),
            pl.BlockSpec(memory_space=pltpu.SMEM),
            pl.BlockSpec((seqs, length, deep), lambda i: (0, 0, i)),
            pl.BlockSpec((deep, width), lambda i: (i, 0)),
            pl.BlockSpec((deep, width), lambda i: (i, 0)),
            pl.BlockSpec((all_heads, deep), lambda i: (0, i)),
            pl.BlockSpec((all_heads, deep), lambda i: (0, i)),
            pl.BlockSpec((seqs, heads, length), lambda i: (0, 0, 0)),
        ],
        out_specs=(pl.BlockSpec(share, lambda i: (0, 0)),) * 2,
        scratch_shapes=[
            pltpu.VMEM((tokens, 2 * width), F32),
            pltpu.VMEM((2 * all_heads, tokens), F32),
            pltpu.VMEM((tokens, width), F32),
            pltpu.VMEM((tokens, width), BF16),
            pltpu.VMEM((tokens, width), BF16),
            pltpu.VMEM((tokens, width), BF16),
            pltpu.VMEM((tokens, width), F32),
            pltpu.VMEM((tokens, width), BF16),
            pltpu.VMEM((tokens, 2 * width), F32),
            pltpu.VMEM((tokens * width // HEAD // 128 * BASE, 128), F32),
            pltpu.VMEM((tokens * width // HEAD // 128 * BASE, 128 * (BASE - 1)), F32),
        ],
        compiler_params=pltpu.CompilerParams(vmem_limit_bytes=63 << 20),
        name="local_maps",
    )(
        place,
        turn,
        logged_fading_speed,
        layer_feed,
        address_mapping,
        content_mapping,
        beta_mapping_matrix.T,
        forgetting_mapping.T,
        extra_forgetting.transpose(0, 2, 1),
    )
    scalar, vector = pl.BlockSpec(memory_space=pltpu.SMEM), pl.BlockSpec(memory_space=pltpu.VMEM)
    small = pltpu.CompilerParams(vmem_limit_bytes=8 << 20)

    def swapped(x, distance):
        return lax.ppermute(x, "sp", [(i, i ^ distance) for i in range(ways)])

    for kernel, distance, lanes, name in ((first_kernel, 1, width, "first"), (second_kernel, 2, width // 2, "second")):
        kept, sent = pl.pallas_call(
            kernel,
            out_shape=(jax.ShapeDtypeStruct((HEAD, lanes), F32),) * 2,
            in_specs=[scalar, vector, vector],
            compiler_params=small,
            name=name,
        )(turn, kept, swapped(sent, distance))
    shares = pl.pallas_call(
        functools.partial(third_kernel, heads),
        out_shape=jax.ShapeDtypeStruct((ways, HEAD // 2, 128), F32),
        in_specs=[scalar, vector, vector, vector],
        compiler_params=small,
        name="third",
    )(turn, opening_probe, kept, swapped(sent, 4))
    mine = lax.all_to_all(shares, "sp", 0, 0, tiled=True)
    return pl.pallas_call(
        result_kernel,
        out_shape=(
            jax.ShapeDtypeStruct((seqs, heads, HEAD // ways, HEAD), BF16),
            jax.ShapeDtypeStruct((seqs, width), BF16),
        ),
        compiler_params=pltpu.CompilerParams(vmem_limit_bytes=8 << 20),
        name="results",
    )(mine)


def solution(mesh):
    in_specs = (
        P("grp", "sp", None),
        P(None, "tp"),
        P(None, "tp"),
        P(),
        P(),
        P("tp"),
        P("grp", "sp", "tp"),
        P("grp", "tp"),
    )
    out_specs = (P("grp", "tp", "sp", None), P("grp", "tp"))
    return jax.shard_map(body, mesh=mesh, in_specs=in_specs, out_specs=out_specs, check_vma=False)
```
